32 devices in a mesh: tp: 8 (over z, x), dp: 4 (over y, core).
Axes of the slice: x: 2, y: 2, z: 4, core: 2. Of those that a mesh axis runs over, the one named last changes fastest.
Arguments:
- tokens: bfloat16 [128, 4096], P('tp', 'dp'), may hold values from -6 to 6
- query_weight: bfloat16 [2, 4096, 2048], P(None, 'dp', 'tp'), may hold values from -0.09375 to 0.09375
- key_weight: bfloat16 [2, 4096, 2048], P(None, 'dp', 'tp'), may hold values from -0.09375 to 0.09375
- value_weight: bfloat16 [2, 4096, 2048], P(None, 'dp', 'tp'), may hold values from -0.09375 to 0.09375
- outgate_weight: bfloat16 [2, 4096, 2048], P(None, 'dp', 'tp'), may hold values from -0.09375 to 0.09375
- igate_weight: bfloat16 [2, 4096, 16], replicated, may hold values from -0.09375 to 0.09375
- fgate_weight: bfloat16 [2, 4096, 16], replicated, may hold values from -0.09375 to 0.09375
- norm_gain: float32 [2, 4096], P(None, 'dp'), may hold values from 0.1 to 1.9
- head_gain: float32 [2, 2048], P(None, 'tp'), may hold values from 0.1 to 1.9
- proj_weight: bfloat16 [2, 2048, 4096], P(None, 'tp', 'dp'), may hold values from -0.125 to 0.125
- cell_state: float32 [2, 128, 16, 128, 128], P(None, 'dp', 'tp'), may hold values from -1.8 to 1.8
- normer_state: float32 [2, 128, 16, 128], P(None, 'dp', 'tp'), may hold values from -1.8 to 1.8
- stab_state: float32 [2, 128, 16], P(None, 'dp', 'tp'), may hold values from -4 to 4
Outputs:
- final_rows: bfloat16 [128, 4096], P('tp', 'dp')
- cell_out: float32 [2, 128, 16, 128, 128], P(None, 'dp', 'tp')
- normer_out: float32 [2, 128, 16, 128], P(None, 'dp', 'tp')
- stab_out: float32 [2, 128, 16], P(None, 'dp', 'tp')
The draws below stay inside these ranges and needn't reach their ends.
All inputs are finite; a program needn't handle non-finite values.
Results may differ from the reference program's by a relative error of at most 0.012.
The reference program's roundings to bfloat16 on the way count: a program that leaves them out, or rounds other values in their place, can miss the bound.
Values may be sent and summed in bfloat16 or wider, within the bound.
A program may use at most 64 MiB of HBM per device.

```python
import jax
import jax.numpy as jnp
from jax import lax

D = 4096
HEADS = 16
DH = 128
BLOCKS = 2
INNER = 2048
BATCH = 128


def block_levels(own_key, dims, shards, least, top_value):
    def one(axis_at, shards_of):
        draws = jax.random.uniform(jax.random.fold_in(jax.random.fold_in(own_key, 6), axis_at), (shards_of,), jnp.float32, least / len(shards), top_value / len(shards))
        return jnp.repeat(jnp.exp(draws), dims[axis_at] // shards_of).reshape((-1,) + (1,) * (len(dims) - axis_at - 1))

    gain = one(*shards[0])
    for cut in shards[1:]:
        gain = gain * one(*cut)
    return gain


def centred(key, extent, deviation, bound, split=(), held_as=jnp.bfloat16):
    entries = deviation * jax.random.normal(key, extent, jnp.float32)
    if split:
        entries = entries * block_levels(key, extent, split, -0.22, 0.18)
    return jnp.clip(entries, -bound, bound).astype(held_as)


def setup_inputs(seed: int = 0) -> dict:
    key_of = jax.random.split(jax.random.key(seed), 14)
    return {
        "tokens": centred(key_of[0], (BATCH, D), 1.0, 6.0, ((0, 8), (1, 4))),
        "query_weight": centred(key_of[1], (BLOCKS, D, INNER), D ** -0.5, 0.09375, ((1, 4), (2, 8))),
        "key_weight": centred(key_of[2], (BLOCKS, D, INNER), D ** -0.5, 0.09375, ((1, 4), (2, 8))),
        "value_weight": centred(key_of[3], (BLOCKS, D, INNER), D ** -0.5, 0.09375, ((1, 4), (2, 8))),
        "outgate_weight": centred(key_of[4], (BLOCKS, D, INNER), D ** -0.5, 0.09375, ((1, 4), (2, 8))),
        "igate_weight": centred(key_of[5], (BLOCKS, D, HEADS), D ** -0.5, 0.09375),
        "fgate_weight": centred(key_of[6], (BLOCKS, D, HEADS), D ** -0.5, 0.09375),
        "norm_gain": jnp.clip(1.0 + 0.18 * jax.random.normal(key_of[7], (BLOCKS, D), jnp.float32), 0.1, 1.9),
        "head_gain": jnp.clip(1.0 + 0.18 * jax.random.normal(key_of[8], (BLOCKS, INNER), jnp.float32), 0.1, 1.9),
        "proj_weight": centred(key_of[9], (BLOCKS, INNER, D), INNER ** -0.5, 0.125, ((1, 8), (2, 4))),
        "cell_state": centred(key_of[10], (BLOCKS, BATCH, HEADS, DH, DH), 0.3, 1.8, ((1, 4), (2, 8)), jnp.float32),
        "normer_state": centred(key_of[11], (BLOCKS, BATCH, HEADS, DH), 0.3, 1.8, ((1, 4), (2, 8)), jnp.float32),
        "stab_state": centred(key_of[12], (BLOCKS, BATCH, HEADS), 1.0, 4.0, ((1, 4), (2, 8)), jnp.float32),
    }


EPSILON = 1e-06

def reference(tokens, query_weight, key_weight, value_weight, outgate_weight, igate_weight, fgate_weight, norm_gain, head_gain, proj_weight, cell_state, normer_state, stab_state):
    current = tokens
    batch_rows = tokens.shape[0]
    cell_list = []
    normer_list = []
    stab_list = []
    for layer_num in range(BLOCKS):
        as_float = current.astype(jnp.float32)
        inv_rms = lax.rsqrt(lax.optimization_barrier(jnp.mean(as_float * as_float, axis=1, keepdims=True)) + EPSILON)
        scaled = (as_float * norm_gain[layer_num].astype(jnp.float32)).astype(jnp.bfloat16)

        def product(weight):
            return jnp.dot(scaled, weight, preferred_element_type=jnp.float32) * inv_rms
        query_rows = product(query_weight[layer_num]).reshape(batch_rows, HEADS, DH)
        key_rows = (product(key_weight[layer_num]) * DH ** (-0.5)).reshape(batch_rows, HEADS, DH)
        value_rows = product(value_weight[layer_num]).reshape(batch_rows, HEADS, DH)
        outgate = product(outgate_weight[layer_num])
        igate = product(igate_weight[layer_num])
        forget = jax.nn.log_sigmoid(product(fgate_weight[layer_num]))
        prev_stab = stab_state[layer_num]
        new_stab = jnp.maximum(forget + prev_stab, igate)
        keep_rate = jnp.exp(forget + prev_stab - new_stab)
        write_rate = jnp.exp(igate - new_stab)
        new_cell = keep_rate[..., None, None] * cell_state[layer_num] + write_rate[..., None, None] * value_rows[..., :, None] * key_rows[..., None, :]
        new_normer = keep_rate[..., None] * normer_state[layer_num] + write_rate[..., None] * key_rows
        numerator = jnp.einsum('bhvd,bhd->bhv', new_cell, query_rows, precision=lax.Precision.HIGHEST)
        denominator = jnp.maximum(jnp.abs(lax.optimization_barrier(jnp.sum(new_normer * query_rows, axis=-1))), 1.0)
        readout = numerator / denominator[..., None]
        normed = readout * lax.rsqrt(lax.optimization_barrier(jnp.mean(readout * readout, axis=-1, keepdims=True)) + EPSILON)
        normed = normed * head_gain[layer_num].reshape(HEADS, DH)
        gated_out = (jax.nn.sigmoid(outgate) * normed.reshape(batch_rows, HEADS * DH)).astype(jnp.bfloat16)
        current = jnp.dot(gated_out, proj_weight[layer_num], preferred_element_type=jnp.float32).astype(jnp.bfloat16)
        cell_list.append(new_cell)
        normer_list.append(new_normer)
        stab_list.append(new_stab)
    return (current, jnp.stack(cell_list), jnp.stack(normer_list), jnp.stack(stab_list))
```

```python
import functools
import math

import jax
import jax.numpy as jnp
from jax import lax
from jax.experimental import pallas as pl
from jax.experimental.pallas import tpu as pltpu
from jax.sharding import PartitionSpec as P

EPSILON = 1e-06
F32 = jnp.float32
BF16 = jnp.bfloat16
MESH = pl.DeviceIdType.MESH


def split_axis(size):
    inner = max(f for f in range(1, math.isqrt(size) + 1) if size % f == 0)
    return size // inner, inner


def row_block(index, rows):
    return pl.ds(pl.multiple_of(index * rows, rows), rows)


def gate_dot(scaled, weight):
    return lax.dot_general(
        scaled, weight, (((1,), (1,)), ((), ())), preferred_element_type=F32
    )


def step_kernel(
    ntp,
    ndp,
    tokens,
    wq,
    wk,
    wv,
    wo,
    wig,
    wfg,
    norm_gain,
    head_gain,
    proj,
    cell,
    normer,
    stab,
    final_out,
    cell_buf,
    normer_out,
    stab_out,
    w_buf,
    ig_buf,
    fg_buf,
    proj_buf,
    written_buf,
    key_buf,
    keep_buf,
    tok_sem,
    small_sem,
    gain_buf,
    head_buf,
    normer_buf,
    stab_buf,
    split_buf,
    current,
    partial,
    gates,
    pair_recv,
    pair_gate,
    pair_sum,
    pair_gsum,
    proj_recv,
    gate_recv,
    gated_all,
    out_part,
    out_stage,
    out_recv,
    load_sem,
    cell_sem,
    ag_send,
    ag_recv,
    pr_send,
    pr_recv,
    pg_send,
    pg_recv,
    rs_send,
    rs_recv,
    gt_send,
    gt_recv,
    gg_send,
    gg_recv,
    os_send,
    os_recv,
):
    blocks = wq.shape[0]
    width, inner = wq.shape[1], wq.shape[2]
    all_heads = wig.shape[1]
    seqs, heads, dh = cell.shape[1], cell.shape[2], cell.shape[3]
    rows = tokens.shape[0]
    t = lax.axis_index("tp")
    d = lax.axis_index("dp")
    outer, side = split_axis(ntp)
    z = t // side
    x = lax.rem(t, side)

    pair = 2 if ndp % 2 == 0 else 1
    ring = ndp // pair
    y = d // pair
    core = lax.rem(d, pair)

    tok_load = pltpu.make_async_copy(tokens, current.at[0, row_block(t, rows)], tok_sem)
    tok_load.start()
    small = [
        pltpu.make_async_copy(src, dst, small_sem.at[i])
        for i, (src, dst) in enumerate(
            (
                (norm_gain, gain_buf),
                (head_gain, head_buf),
                (normer, normer_buf),
                (stab, stab_buf),
            )
        )
    ]
    loads = []
    for b in range(blocks):
        for i, w in enumerate((wq, wk, wv, wo)):
            loads.append(pltpu.make_async_copy(w.at[b], w_buf.at[b, i], load_sem.at[b, i]))
        loads.append(
            pltpu.make_async_copy(
                wig.at[b, :, row_block(d, width)], ig_buf.at[b], load_sem.at[b, 4]
            )
        )
        loads.append(
            pltpu.make_async_copy(
                wfg.at[b, :, row_block(d, width)], fg_buf.at[b], load_sem.at[b, 5]
            )
        )
        loads.append(pltpu.make_async_copy(proj.at[b], proj_buf.at[b], load_sem.at[b, 6]))
    cell_loads = [
        pltpu.make_async_copy(cell.at[b], cell_buf.at[b], cell_sem.at[b]) for b in range(blocks)
    ]
    per_block = 7
    for b in range(blocks):
        for c in loads[b * per_block : (b + 1) * per_block]:
            c.start()
        cell_loads[b].start()
        if b == 0:
            for c in small:
                c.start()

    barrier = pltpu.get_barrier_semaphore()
    for k in range(1, ntp):
        pl.semaphore_signal(
            barrier, inc=1, device_id={"tp": lax.rem(t + k, ntp)}, device_id_type=MESH
        )
    for k in range(1, ndp):
        pl.semaphore_signal(
            barrier, inc=1, device_id={"dp": lax.rem(d + k, ndp)}, device_id_type=MESH
        )
    pl.semaphore_wait(barrier, ntp - 1 + ndp - 1)
    tok_load.wait()

    def split_cells(b):
        cell_loads[b].wait()

        def one(i, _):
            for h in range(heads):
                whole = cell_buf[b, i, h]
                high = whole.astype(BF16)
                here = row_block(i, dh)
                split_buf[h, here, 0:dh] = high
                split_buf[h, here, dh : 2 * dh] = (whole - high.astype(F32)).astype(BF16)
            return 0

        lax.fori_loop(0, seqs, one, 0)

    eight = math.gcd(seqs, 8)

    def update_cells(b):
        def one(c, _):
            here = row_block(c, eight)
            keep = keep_buf[here, :]
            for h in range(heads):
                lanes = slice(h * dh, (h + 1) * dh)
                across = jnp.transpose(written_buf[here, lanes])
                keys = key_buf[here, lanes]
                for j in range(eight):
                    cell_buf[b, c * eight + j, h] = (
                        keep[j : j + 1, h : h + 1] * cell_buf[b, c * eight + j, h]
                        + across[:, j : j + 1] * keys[j : j + 1, :]
                    )
            return 0

        lax.fori_loop(0, seqs // eight, one, 0)

    def gather(b):
        buf = current.at[b]
        own_src = buf.at[row_block(t, rows)]

        def send(src, block, slot, dest):
            copy = pltpu.make_async_remote_copy(
                src_ref=src,
                dst_ref=buf.at[row_block(block, rows)],
                send_sem=ag_send.at[b, slot],
                recv_sem=ag_recv.at[b, slot],
                device_id={"tp": dest},
                device_id_type=MESH,
            )
            copy.start()
            return copy

        first, second = [], []
        for k in range(1, outer):
            dest = lax.rem(z + k, outer) * side + x
            first.append(send(own_src, t, k - 1, dest))
        for j in range(1, side):
            dest = z * side + lax.rem(x + j, side)
            second.append(send(own_src, t, outer - 1 + (j - 1) * outer, dest))
        if b == 0:
            split_cells(0)
            for c in small:
                c.wait()
        for k in range(1, outer):
            first[k - 1].wait_recv()
            block = lax.rem(z - k + outer, outer) * side + x
            for j in range(1, side):
                dest = z * side + lax.rem(x + j, side)
                second.append(
                    send(
                        buf.at[row_block(block, rows)],
                        block,
                        outer - 1 + (j - 1) * outer + k,
                        dest,
                    )
                )
        for c in second:
            c.wait_recv()
        for c in first + second:
            c.wait_send()

    for b in range(blocks):
        gather(b)
        for c in loads[b * per_block : (b + 1) * per_block]:
            c.wait()
        as_float = current[b].astype(F32)
        scaled = (as_float * gain_buf[b : b + 1, :]).astype(BF16)
        gates[b, :, 0:all_heads] = gate_dot(scaled, ig_buf[b])
        gates[b, :, all_heads : 2 * all_heads] = gate_dot(scaled, fg_buf[b])
        gates[b, :, 2 * all_heads : 2 * all_heads + 1] = jnp.sum(
            as_float * as_float, axis=1, keepdims=True
        )
        sends = []

        def send_rows(srcs, dsts, send_sems, recv_sems, slot, dest):
            started = []
            for src, dst, ss, rr in zip(srcs, dsts, send_sems, recv_sems):
                copy = pltpu.make_async_remote_copy(
                    src_ref=src,
                    dst_ref=dst,
                    send_sem=ss.at[b, slot],
                    recv_sem=rr.at[b, slot],
                    device_id={"dp": dest},
                    device_id_type=MESH,
                )
                copy.start()
                started.append(copy)
            sends.extend(started)
            return started

        for i in range(4):
            cols = slice(i * inner, (i + 1) * inner)
            partial[b, :, cols] = jnp.dot(scaled, w_buf[b, i], preferred_element_type=F32)
        paired = []
        if pair == 2:
            mate = y * pair + 1 - core
            for k in range(ring):
                slot = (k + 1) % ring
                block = row_block(lax.rem(y + slot, ring) * pair + 1 - core, seqs)
                paired.append(
                    (
                        slot,
                        send_rows(
                            (partial.at[b, block], gates.at[b, block]),
                            (pair_recv.at[b, slot], pair_gate.at[b, slot]),
                            (pr_send, pg_send),
                            (pr_recv, pg_recv),
                            slot,
                            mate,
                        ),
                    )
                )
        else:
            paired = [((k + 1) % ring, []) for k in range(ring)]
        arriving = []
        total = gate_sum = None
        for slot, copies in paired:
            for c in copies:
                c.wait_recv()
            dest = lax.rem(y + slot, ring) * pair + core
            block = row_block(dest, seqs)
            rows_sum, gsum = partial[b, block, :], gates[b, block, :]
            if copies:
                rows_sum = rows_sum + pair_recv[b, slot]
                gsum = gsum + pair_gate[b, slot]
            if slot == 0:
                total, gate_sum = rows_sum, gsum
            else:
                pair_sum[b, slot - 1] = rows_sum.astype(pair_sum.dtype)
                pair_gsum[b, slot - 1] = gsum
                arriving.append(
                    send_rows(
                        (pair_sum.at[b, slot - 1], pair_gsum.at[b, slot - 1]),
                        (proj_recv.at[b, slot - 1], gate_recv.at[b, slot - 1]),
                        (rs_send, gt_send),
                        (rs_recv, gt_recv),
                        slot - 1,
                        dest,
                    )
                )
        for k in range(ring - 1):
            for c in arriving[k]:
                c.wait_recv()
            total = total + proj_recv[b, k].astype(F32)
            gate_sum = gate_sum + gate_recv[b, k]
        own = row_block(d, seqs)
        inv_rms = lax.rsqrt(gate_sum[:, 2 * all_heads : 2 * all_heads + 1] / (width * ndp) + EPSILON)
        query = total[:, 0:inner] * inv_rms
        key = total[:, inner : 2 * inner] * inv_rms * (dh ** (-0.5))
        value = total[:, 2 * inner : 3 * inner] * inv_rms
        outgate = total[:, 3 * inner : 4 * inner] * inv_rms
        pre = gate_sum * inv_rms
        key_buf[...] = key
        wide = -(-2 * seqs // 128) * 128
        column = lax.broadcasted_iota(jnp.int32, (dh, wide), 1)
        reads = []
        for h in range(heads):
            lanes = slice(h * dh, (h + 1) * dh)
            high = query[:, lanes].astype(BF16)
            low = (query[:, lanes] - high.astype(F32)).astype(BF16)
            terms = [jnp.concatenate([a, a], 1) for a in (high, low)]
            if wide > 2 * seqs:
                terms.append(jnp.zeros((wide - 2 * seqs, 2 * dh), BF16))
            rhs = jnp.concatenate(terms, 0)
            acc = jnp.zeros((dh, wide), F32)
            for c in range(seqs // eight):
                prod = gate_dot(
                    split_buf[h, c * eight * dh : (c + 1) * eight * dh, :], rhs
                )
                for j in range(eight):
                    own_column = (column == c * eight + j) | (column == seqs + c * eight + j)
                    acc = jnp.where(own_column, prod[j * dh : (j + 1) * dh], acc)
            turned = jnp.transpose(acc)
            reads.append(turned[0:seqs] + turned[seqs : 2 * seqs])

        lane = lax.broadcasted_iota(jnp.int32, pre.shape, 1)
        aux = jnp.zeros(pre.shape, F32)
        for h in range(heads):
            lanes = slice(h * dh, (h + 1) * dh)
            head = t * heads + h
            igate = jnp.sum(jnp.where(lane == head, pre, 0.0), axis=1, keepdims=True)
            fpre = jnp.sum(jnp.where(lane == head + all_heads, pre, 0.0), axis=1, keepdims=True)
            lf = jnp.minimum(fpre, 0.0) - jnp.log1p(jnp.exp(-jnp.abs(fpre)))
            stab_row = jnp.broadcast_to(stab_buf[b, h : h + 1, :], (seqs, seqs))
            diag = lax.broadcasted_iota(jnp.int32, (seqs, seqs), 0) == (
                lax.broadcasted_iota(jnp.int32, (seqs, seqs), 1)
            )
            m0 = jnp.sum(jnp.where(diag, stab_row, 0.0), axis=1, keepdims=True)
            carried = lf + m0
            m1 = jnp.maximum(carried, igate)
            stab_out[b, h : h + 1, :] = jnp.sum(jnp.where(diag, m1, 0.0), axis=0, keepdims=True)
            keep = jnp.exp(carried - m1)
            write = jnp.exp(igate - m1)
            qh, kh = query[:, lanes], key[:, lanes]
            written = write * value[:, lanes]
            n1 = keep * normer_buf[b, :, h, :] + write * kh
            written_buf[:, lanes] = written
            normer_out[b, :, h, :] = n1
            aux = jnp.where(lane == h, keep, aux)
            numer = keep * reads[h] + written * jnp.sum(kh * qh, axis=1, keepdims=True)
            denom = jnp.maximum(jnp.abs(jnp.sum(n1 * qh, axis=1, keepdims=True)), 1.0)
            readout = numer / denom
            normed = readout * lax.rsqrt(
                jnp.mean(readout * readout, axis=1, keepdims=True) + EPSILON
            )
            normed = normed * head_buf[b : b + 1, lanes]
            gate = 1.0 / (1.0 + jnp.exp(-outgate[:, lanes]))
            gated_all[b, own, lanes] = (gate * normed).astype(BF16)
        keep_buf[...] = aux

        spread = []
        for k in range(1, ndp):
            copy = pltpu.make_async_remote_copy(
                src_ref=gated_all.at[b, own],
                dst_ref=gated_all.at[b, own],
                send_sem=gg_send.at[b, k - 1],
                recv_sem=gg_recv.at[b, k - 1],
                device_id={"dp": lax.rem(d + k, ndp)},
                device_id_type=MESH,
            )
            copy.start()
            spread.append(copy)
        for c in spread:
            c.wait_recv()
        part = jnp.dot(gated_all[b], proj_buf[b], preferred_element_type=F32)
        out_part[...] = part
        out_stage[b] = part.astype(BF16)
        outs = []
        for k in range(1, ntp):
            dest = lax.rem(t + k, ntp)
            copy = pltpu.make_async_remote_copy(
                src_ref=out_stage.at[b, row_block(dest, rows)],
                dst_ref=out_recv.at[b, k - 1],
                send_sem=os_send.at[b, k - 1],
                recv_sem=os_recv.at[b, k - 1],
                device_id={"tp": dest},
                device_id_type=MESH,
            )
            copy.start()
            outs.append(copy)
        update_cells(b)
        if b + 1 < blocks:
            split_cells(b + 1)
        for c in outs:
            c.wait_recv()
        summed = out_part[row_block(t, rows), :]
        for k in range(ntp - 1):
            summed = summed + out_recv[b, k].astype(F32)
        if b + 1 < blocks:
            current[b + 1, row_block(t, rows), :] = summed.astype(BF16)
        else:
            final_out[...] = summed.astype(BF16)
        for c in sends + spread + outs:
            c.wait_send()


def store_kernel(rows, cell, normer, stab, rows_out, cell_out, normer_out, stab_out, cell_sem, sems):
    blocks, seqs = cell.shape[0], cell.shape[1]
    parts = cell_sem.shape[1]
    step = seqs // parts
    copies = [
        pltpu.make_async_copy(
            cell.at[b, i * step : (i + 1) * step],
            cell_out.at[b, i * step : (i + 1) * step],
            cell_sem.at[b, i],
        )
        for b in range(blocks)
        for i in range(parts)
    ]
    for i, (src, dst) in enumerate(((rows, rows_out), (normer, normer_out), (stab, stab_out))):
        copies.append(pltpu.make_async_copy(src, dst, sems.at[i]))
    for c in copies:
        c.start()
    for c in copies:
        c.wait()


def per_device(ntp, ndp, *args):
    (tokens, wq, wk, wv, wo, wig, wfg, norm_gain, head_gain, proj, cell, normer, stab) = args
    blocks, width, inner = wq.shape
    all_heads = wig.shape[2]
    seqs, heads, dh = cell.shape[1], cell.shape[2], cell.shape[3]
    rows = tokens.shape[0]
    pair = 2 if ndp % 2 == 0 else 1
    ring = ndp // pair
    more = max(ring - 1, 1)
    wig, wfg, stab = (jnp.swapaxes(a, 1, 2) for a in (wig, wfg, stab))
    batch = rows * ntp
    lanes = -(-(2 * all_heads + 1) // 128) * 128
    vmem = pl.BlockSpec(memory_space=pltpu.VMEM)
    hbm = pl.BlockSpec(memory_space=pltpu.HBM)
    dma = pltpu.SemaphoreType.DMA
    results = pl.pallas_call(
        functools.partial(step_kernel, ntp, ndp),
        out_shape=(
            pltpu.VMEM(tokens.shape, BF16),
            pltpu.VMEM(cell.shape, F32),
            pltpu.VMEM(normer.shape, F32),
            pltpu.VMEM(stab.shape, F32),
        ),
        in_specs=[hbm] * 13,
        out_specs=(vmem,) * 4,
        scratch_shapes=[
            pltpu.VMEM((blocks, 4, width, inner), BF16),
            pltpu.VMEM((blocks, all_heads, width), BF16),
            pltpu.VMEM((blocks, all_heads, width), BF16),
            pltpu.VMEM(proj.shape, BF16),
            pltpu.VMEM((seqs, inner), F32),
            pltpu.VMEM((seqs, inner), F32),
            pltpu.VMEM((seqs, lanes), F32),
            dma,
            dma((4,)),
            pltpu.VMEM(norm_gain.shape, F32),
            pltpu.VMEM(head_gain.shape, F32),
            pltpu.VMEM(normer.shape, F32),
            pltpu.VMEM(stab.shape, F32),
            pltpu.VMEM((heads, seqs * dh, 2 * dh), BF16),
            pltpu.VMEM((blocks, batch, width), BF16),
            pltpu.VMEM((blocks, batch, 4 * inner), F32),
            pltpu.VMEM((blocks, batch, lanes), F32),
            pltpu.VMEM((blocks, ring, seqs, 4 * inner), F32),
            pltpu.VMEM((blocks, ring, seqs, lanes), F32),
            pltpu.VMEM((blocks, more, seqs, 4 * inner), F32),
            pltpu.VMEM((blocks, more, seqs, lanes), F32),
            pltpu.VMEM((blocks, more, seqs, 4 * inner), F32),
            pltpu.VMEM((blocks, more, seqs, lanes), F32),
            pltpu.VMEM((blocks, batch, inner), BF16),
            pltpu.VMEM((batch, width), F32),
            pltpu.VMEM((blocks, batch, width), BF16),
            pltpu.VMEM((blocks, ntp - 1, rows, width), BF16),
            dma((blocks, 7)),
            dma((blocks,)),
            dma((blocks, ntp - 1)),
            dma((blocks, ntp - 1)),
            dma((blocks, ring)),
            dma((blocks, ring)),
            dma((blocks, ring)),
            dma((blocks, ring)),
            dma((blocks, more)),
            dma((blocks, more)),
            dma((blocks, more)),
            dma((blocks, more)),
            dma((blocks, ndp - 1)),
            dma((blocks, ndp - 1)),
            dma((blocks, ntp - 1)),
            dma((blocks, ntp - 1)),
        ],
        compiler_params=pltpu.CompilerParams(
            collective_id=0, has_side_effects=True, vmem_limit_bytes=40 << 20
        ),
    )(
        *[
            pltpu.with_memory_space_constraint(a, pltpu.HBM)
            for a in (
                tokens, wq, wk, wv, wo, wig, wfg, norm_gain, head_gain, proj, cell, normer, stab
            )
        ]
    )

    shapes = tuple(jax.ShapeDtypeStruct(a.shape, a.dtype) for a in results)
    rows_out, cell_out, normer_out, stab_out = pl.pallas_call(
        store_kernel,
        out_shape=shapes,
        in_specs=[vmem] * 4,
        out_specs=(hbm,) * 4,
        scratch_shapes=[dma((blocks, math.gcd(seqs, 8))), dma((3,))],
        compiler_params=pltpu.CompilerParams(vmem_limit_bytes=1 << 20),
    )(*results)
    return rows_out, cell_out, normer_out, jnp.swapaxes(stab_out, 1, 2)


def solution(mesh):
    return jax.shard_map(
        functools.partial(per_device, mesh.shape["tp"], mesh.shape["dp"]),
        mesh=mesh,
        in_specs=(
            P("tp", "dp"),
            P(None, "dp", "tp"),
            P(None, "dp", "tp"),
            P(None, "dp", "tp"),
            P(None, "dp", "tp"),
            P(),
            P(),
            P(None, "dp"),
            P(None, "tp"),
            P(None, "tp", "dp"),
            P(None, "dp", "tp", None, None),
            P(None, "dp", "tp", None),
            P(None, "dp", "tp"),
        ),
        out_specs=(
            P("tp", "dp"),
            P(None, "dp", "tp", None, None),
            P(None, "dp", "tp", None),
            P(None, "dp", "tp"),
        ),
        check_vma=False,
    )
```

```python
import functools
import math

import jax
import jax.numpy as jnp
from jax import lax
from jax.experimental import pallas as pl
from jax.experimental.pallas import tpu as pltpu
from jax.sharding import PartitionSpec as P

EPSILON = 1e-06
F32 = jnp.float32
BF16 = jnp.bfloat16
MESH = pl.DeviceIdType.MESH


def split_axis(size):
    inner = max(f for f in range(1, math.isqrt(size) + 1) if size % f == 0)
    return size // inner, inner


def row_block(index, rows):
    return pl.ds(pl.multiple_of(index * rows, rows), rows)


def gate_dot(scaled, weight):
    return lax.dot_general(
        scaled, weight, (((1,), (1,)), ((), ())), preferred_element_type=F32
    )


def line_order(pos, size):
    low = jnp.minimum(pos, size - 1 - pos)
    order = []
    for k in range(1, size):
        step = (k + 1) // 2
        near = pos + (step if k % 2 == 0 else -step)
        far = jnp.where(2 * pos < size - 1, pos + k - low, pos - k + low)
        order.append(jnp.where(k <= 2 * low, near, far))
    return order


def step_kernel(
    ntp,
    ndp,
    tokens,
    wq,
    wk,
    wv,
    wo,
    wig,
    wfg,
    norm_gain,
    head_gain,
    proj,
    cell,
    normer,
    stab,
    final_out,
    cell_buf,
    normer_out,
    stab_out,
    w_buf,
    ig_buf,
    fg_buf,
    proj_buf,
    written_buf,
    key_buf,
    keep_buf,
    tok_sem,
    small_sem,
    gain_buf,
    head_buf,
    normer_buf,
    stab_buf,
    split_buf,
    current,
    scaled_buf,
    partial,
    gates,
    gate_recv,
    gate_cols,
    pair_recv,
    pair_sum,
    proj_recv,
    gated_all,
    out_part,
    out_stage,
    out_recv,
    load_sem,
    cell_sem,
    ag_send,
    ag_recv,
    pr_send,
    pr_recv,
    rs_send,
    rs_recv,
    gt_send,
    gt_recv,
    gg_send,
    gg_recv,
    os_send,
    os_recv,
):
    blocks = wq.shape[0]
    width, inner = wq.shape[1], wq.shape[2]
    all_heads = wig.shape[1]
    seqs, heads, dh = cell.shape[1], cell.shape[2], cell.shape[3]
    rows = tokens.shape[0]
    batch = rows * ntp
    t = lax.axis_index("tp")
    d = lax.axis_index("dp")
    outer, side = split_axis(ntp)
    z = t // side
    x = lax.rem(t, side)
    z_order = line_order(z, outer)

    pair = 2 if ndp % 2 == 0 else 1
    ring = ndp // pair
    y = d // pair
    core = lax.rem(d, pair)
    own = row_block(d, seqs)
    mine = row_block(t, rows)

    tok_load = pltpu.make_async_copy(tokens, current.at[0, mine], tok_sem)
    tok_load.start()
    barrier = pltpu.get_barrier_semaphore()
    for k in range(1, ntp):
        pl.semaphore_signal(
            barrier, inc=1, device_id={"tp": lax.rem(t + k, ntp)}, device_id_type=MESH
        )
    for k in range(1, ndp):
        pl.semaphore_signal(
            barrier, inc=1, device_id={"dp": lax.rem(d + k, ndp)}, device_id_type=MESH
        )
    small = [
        pltpu.make_async_copy(src, dst, small_sem.at[i])
        for i, (src, dst) in enumerate(
            (
                (norm_gain, gain_buf),
                (head_gain, head_buf),
                (normer, normer_buf),
                (stab, stab_buf),
            )
        )
    ]
    loads = []
    for b in range(blocks):
        one = [
            pltpu.make_async_copy(w.at[b], w_buf.at[b, i], load_sem.at[b, i])
            for i, w in enumerate((wq, wk, wv, wo))
        ]
        one.append(
            pltpu.make_async_copy(
                wig.at[b, :, row_block(d, width)], ig_buf.at[b], load_sem.at[b, 4]
            )
        )
        one.append(
            pltpu.make_async_copy(
                wfg.at[b, :, row_block(d, width)], fg_buf.at[b], load_sem.at[b, 5]
            )
        )
        one.append(pltpu.make_async_copy(proj.at[b], proj_buf.at[b], load_sem.at[b, 6]))
        loads.append(one)
    cell_loads = [
        pltpu.make_async_copy(cell.at[b], cell_buf.at[b], cell_sem.at[b]) for b in range(blocks)
    ]
    tok_load.wait()
    for c in small:
        c.start()
    for b in range(blocks):
        for c in loads[b]:
            c.start()
        cell_loads[b].start()
    pl.semaphore_wait(barrier, ntp - 1 + ndp - 1)

    def split_cells(b):
        cell_loads[b].wait()

        def one(i, _):
            for h in range(heads):
                whole = cell_buf[b, i, h]
                high = whole.astype(BF16)
                here, lanes = row_block(i, dh), slice(h * dh, (h + 1) * dh)
                split_buf[0, here, lanes] = high
                split_buf[1, here, lanes] = (whole - high.astype(F32)).astype(BF16)
            return 0

        lax.fori_loop(0, seqs, one, 0)

    eight = math.gcd(seqs, 8)

    def update_cells(b):
        def one(c, _):
            here = row_block(c, eight)
            keep = keep_buf[here, :]
            for h in range(heads):
                lanes = slice(h * dh, (h + 1) * dh)
                across = jnp.transpose(written_buf[here, lanes])
                keys = key_buf[here, lanes]
                for j in range(eight):
                    cell_buf[b, c * eight + j, h] = (
                        keep[j : j + 1, h : h + 1] * cell_buf[b, c * eight + j, h]
                        + across[:, j : j + 1] * keys[j : j + 1, :]
                    )
            return 0

        lax.fori_loop(0, seqs // eight, one, 0)

    def ag_copy(b, block, slot, dest):
        here = row_block(block, rows)
        return pltpu.make_async_remote_copy(
            src_ref=current.at[b, here],
            dst_ref=current.at[b, here],
            send_sem=ag_send.at[b, slot],
            recv_sem=ag_recv.at[b, slot],
            device_id={"tp": dest},
            device_id_type=MESH,
        )

    def gather_start(b):
        sent = []
        for zd in reversed(z_order):
            sent.append(ag_copy(b, t, lax.rem(zd - z + outer, outer) - 1, zd * side + x))
        for j in range(1, side):
            dest = z * side + lax.rem(x + j, side)
            sent.append(ag_copy(b, t, outer - 1 + (j - 1) * outer, dest))
        for c in sent:
            c.start()
        return sent

    def gather_finish(b, sent):
        for zs in z_order:
            gap = lax.rem(z - zs + outer, outer)
            block = zs * side + x
            ag_copy(b, block, gap - 1, block).wait_recv()
            for j in range(1, side):
                dest = z * side + lax.rem(x + j, side)
                copy = ag_copy(b, block, outer - 1 + (j - 1) * outer + gap, dest)
                copy.start()
                sent.append(copy)
        for j in range(1, side):
            xs = lax.rem(x - j + side, side)
            from_x = z * side + xs
            ag_copy(b, from_x, outer - 1 + (j - 1) * outer, from_x).wait_recv()
            for zs in z_order:
                gap = lax.rem(z - zs + outer, outer)
                slot = outer - 1 + (j - 1) * outer + gap
                ag_copy(b, zs * side + xs, slot, from_x).wait_recv()
        return sent

    gather = gather_start(0)
    for b in range(blocks):
        if b == 0:
            split_cells(0)
            for c in small:
                c.wait()
        sends = gather_finish(b, gather)
        as_float = current[b].astype(F32)
        scaled_buf[...] = (as_float * gain_buf[b : b + 1, :]).astype(BF16)

        def dp_send(src, dst, send_sem, recv_sem, dest):
            copy = pltpu.make_async_remote_copy(
                src_ref=src,
                dst_ref=dst,
                send_sem=send_sem,
                recv_sem=recv_sem,
                device_id={"dp": dest},
                device_id_type=MESH,
            )
            copy.start()
            sends.append(copy)
            return copy

        mate = y * pair + (pair - 1 - core)
        paired = []
        for i in range(4):
            loads[b][i].wait()
            partial[b, i] = jnp.dot(scaled_buf[...], w_buf[b, i], preferred_element_type=F32)
            one = {}
            if pair == 2:
                for k in range(ring):
                    slot = (k + 1) % ring
                    block = row_block(lax.rem(y + slot, ring) * pair + 1 - core, seqs)
                    one[slot] = dp_send(
                        partial.at[b, i, block],
                        pair_recv.at[b, i, slot],
                        pr_send.at[b, i, slot],
                        pr_recv.at[b, i, slot],
                        mate,
                    )
            paired.append(one)

        for c in loads[b][4:]:
            c.wait()
        square = as_float * as_float
        high = square.astype(BF16)
        low = (square - high.astype(F32)).astype(BF16)
        ones = jnp.ones((16, width), BF16)
        squares = gate_dot(ones, high) + gate_dot(ones, low)
        igates = gate_dot(ig_buf[b], scaled_buf[...])
        fgates = gate_dot(fg_buf[b], scaled_buf[...])
        head_row = lax.broadcasted_iota(jnp.int32, (all_heads, batch), 0)
        lines = []
        for source in (igates, fgates):
            for h in range(heads):
                hit = head_row == t * heads + h
                lines.append(jnp.sum(jnp.where(hit, source, 0.0), axis=0, keepdims=True))
        lines.append(squares[0:1])
        line = lax.broadcasted_iota(jnp.int32, gates.shape[1:], 0)
        packed = jnp.zeros(gates.shape[1:], F32)
        for r, value in enumerate(lines):
            packed = jnp.where(line == r, jnp.broadcast_to(value, packed.shape), packed)
        gates[b] = packed
        gate_copies = []
        for k in sorted(range(1, ndp), key=lambda k: -min(k, ndp - k)):
            gate_copies.append(
                dp_send(
                    gates.at[b],
                    gate_recv.at[b, k - 1],
                    gt_send.at[b, k - 1],
                    gt_recv.at[b, k - 1],
                    lax.rem(d + k, ndp),
                )
            )

        arriving = []
        for i in range(4):
            one = []
            for slot in range(1, ring):
                dest = lax.rem(y + slot, ring) * pair + core
                summed = partial[b, i, row_block(dest, seqs), :]
                if pair == 2:
                    paired[i][slot].wait_recv()
                    summed = summed + pair_recv[b, i, slot]
                pair_sum[b, i, slot - 1] = summed
                one.append(
                    dp_send(
                        pair_sum.at[b, i, slot - 1],
                        proj_recv.at[b, i, slot - 1],
                        rs_send.at[b, i, slot - 1],
                        rs_recv.at[b, i, slot - 1],
                        dest,
                    )
                )
            arriving.append(one)

        for c in gate_copies:
            c.wait_recv()
        gate_sum = gates[b]
        for k in range(ndp - 1):
            gate_sum = gate_sum + gate_recv[b, k]
        gate_cols[...] = jnp.transpose(gate_sum)
        pre = gate_cols[own, :]
        inv_rms = lax.rsqrt(pre[:, 2 * heads : 2 * heads + 1] / (width * ndp) + EPSILON)
        pre = pre * inv_rms
        diag = lax.broadcasted_iota(jnp.int32, (seqs, seqs), 0) == (
            lax.broadcasted_iota(jnp.int32, (seqs, seqs), 1)
        )
        lane = lax.broadcasted_iota(jnp.int32, keep_buf.shape, 1)
        aux = jnp.zeros(keep_buf.shape, F32)
        keeps, writes = [], []
        for h in range(heads):
            igate, fpre = pre[:, h : h + 1], pre[:, heads + h : heads + h + 1]
            lf = jnp.minimum(fpre, 0.0) - jnp.log1p(jnp.exp(-jnp.abs(fpre)))
            stab_row = jnp.broadcast_to(stab_buf[b, h : h + 1, :], (seqs, seqs))
            m0 = jnp.sum(jnp.where(diag, stab_row, 0.0), axis=1, keepdims=True)
            carried = lf + m0
            m1 = jnp.maximum(carried, igate)
            stab_out[b, h : h + 1, :] = jnp.sum(jnp.where(diag, m1, 0.0), axis=0, keepdims=True)
            keeps.append(jnp.exp(carried - m1))
            writes.append(jnp.exp(igate - m1))
            aux = jnp.where(lane == h, keeps[h], aux)
        keep_buf[...] = aux

        def total(i):
            value = partial[b, i, own, :]
            if pair == 2:
                paired[i][0].wait_recv()
                value = value + pair_recv[b, i, 0]
            for k in range(ring - 1):
                arriving[i][k].wait_recv()
                value = value + proj_recv[b, i, k]
            return value * inv_rms

        query = total(0)
        wide = -(-2 * heads * seqs // 128) * 128
        column = lax.rem(lax.broadcasted_iota(jnp.int32, (dh, wide), 1), seqs)
        terms = []
        for h in range(heads):
            high = query[:, h * dh : (h + 1) * dh].astype(BF16)
            low = (query[:, h * dh : (h + 1) * dh] - high.astype(F32)).astype(BF16)
            for part in (high, low):
                blank = jnp.zeros(part.shape, BF16)
                terms.append(jnp.concatenate([part if g == h else blank for g in range(heads)], 1))
        if wide > 2 * heads * seqs:
            terms.append(jnp.zeros((wide - 2 * heads * seqs, heads * dh), BF16))
        rhs = jnp.concatenate(terms, 0)
        acc = jnp.zeros((dh, wide), F32)
        for c in range(seqs // eight):
            here = slice(c * eight * dh, (c + 1) * eight * dh)
            prod = gate_dot(split_buf[0, here, :], rhs) + gate_dot(split_buf[1, here, :], rhs)
            for j in range(eight):
                acc = jnp.where(column == c * eight + j, prod[j * dh : (j + 1) * dh], acc)
        turned = jnp.transpose(acc)
        reads = [
            turned[2 * h * seqs : (2 * h + 1) * seqs]
            + turned[(2 * h + 1) * seqs : (2 * h + 2) * seqs]
            for h in range(heads)
        ]
        key = total(1) * (dh ** (-0.5))
        key_buf[...] = key
        dots, normers = [], []
        for h in range(heads):
            lanes = slice(h * dh, (h + 1) * dh)
            qh, kh = query[:, lanes], key[:, lanes]
            n1 = keeps[h] * normer_buf[b, :, h, :] + writes[h] * kh
            normer_out[b, :, h, :] = n1
            dots.append(jnp.sum(kh * qh, axis=1, keepdims=True))
            normers.append(jnp.sum(n1 * qh, axis=1, keepdims=True))
        value = total(2)
        normed = []
        for h in range(heads):
            lanes = slice(h * dh, (h + 1) * dh)
            written = writes[h] * value[:, lanes]
            written_buf[:, lanes] = written
            numer = keeps[h] * reads[h] + written * dots[h]
            readout = numer / jnp.maximum(jnp.abs(normers[h]), 1.0)
            one = readout * lax.rsqrt(jnp.mean(readout * readout, axis=1, keepdims=True) + EPSILON)
            normed.append(one * head_buf[b : b + 1, lanes])
        outgate = total(3)
        for h in range(heads):
            lanes = slice(h * dh, (h + 1) * dh)
            gate = 1.0 / (1.0 + jnp.exp(-outgate[:, lanes]))
            gated_all[b, own, lanes] = (gate * normed[h]).astype(BF16)

        spread = []
        for k in sorted(range(1, ndp), key=lambda k: -min(k, ndp - k)):
            spread.append(
                dp_send(
                    gated_all.at[b, own],
                    gated_all.at[b, own],
                    gg_send.at[b, k - 1],
                    gg_recv.at[b, k - 1],
                    lax.rem(d + k, ndp),
                )
            )
        for c in spread:
            c.wait_recv()
        part = jnp.dot(gated_all[b], proj_buf[b], preferred_element_type=F32)
        out_stage[b] = part.astype(BF16)
        out_part[...] = part
        outs = []
        for zd in list(reversed(z_order)) + [z]:
            for xd in range(1 if zd is z else 0, side):
                dest = zd * side + lax.rem(x + xd, side)
                slot = lax.rem(dest - t + ntp, ntp) - 1
                copy = pltpu.make_async_remote_copy(
                    src_ref=out_stage.at[b, row_block(dest, rows)],
                    dst_ref=out_recv.at[b, slot],
                    send_sem=os_send.at[b, slot],
                    recv_sem=os_recv.at[b, slot],
                    device_id={"tp": dest},
                    device_id_type=MESH,
                )
                copy.start()
                outs.append(copy)
        update_cells(b)
        if b + 1 < blocks:
            split_cells(b + 1)
        for c in outs:
            c.wait_recv()
        summed = out_part[mine, :]
        for k in range(ntp - 1):
            summed = summed + out_recv[b, k].astype(F32)
        if b + 1 < blocks:
            current[b + 1, mine, :] = summed.astype(BF16)
            gather = gather_start(b + 1)
        else:
            final_out[...] = summed.astype(BF16)
        for c in sends + outs:
            c.wait_send()


def store_kernel(rows, cell, normer, stab, rows_out, cell_out, normer_out, stab_out, cell_sem, sems):
    blocks, seqs = cell.shape[0], cell.shape[1]
    parts = cell_sem.shape[1]
    step = seqs // parts
    copies = [
        pltpu.make_async_copy(
            cell.at[b, i * step : (i + 1) * step],
            cell_out.at[b, i * step : (i + 1) * step],
            cell_sem.at[b, i],
        )
        for b in range(blocks)
        for i in range(parts)
    ]
    for i, (src, dst) in enumerate(((rows, rows_out), (normer, normer_out), (stab, stab_out))):
        copies.append(pltpu.make_async_copy(src, dst, sems.at[i]))
    for c in copies:
        c.start()
    for c in copies:
        c.wait()


def per_device(ntp, ndp, *args):
    (tokens, wq, wk, wv, wo, wig, wfg, norm_gain, head_gain, proj, cell, normer, stab) = args
    blocks, width, inner = wq.shape
    all_heads = wig.shape[2]
    seqs, heads, dh = cell.shape[1], cell.shape[2], cell.shape[3]
    rows = tokens.shape[0]
    pair = 2 if ndp % 2 == 0 else 1
    ring = ndp // pair
    more = max(ring - 1, 1)
    wig, wfg, stab = (jnp.swapaxes(a, 1, 2) for a in (wig, wfg, stab))
    batch = rows * ntp
    lanes = -(-heads // 128) * 128
    gate_rows = -(-(2 * heads + 1) // 8) * 8
    vmem = pl.BlockSpec(memory_space=pltpu.VMEM)
    hbm = pl.BlockSpec(memory_space=pltpu.HBM)
    dma = pltpu.SemaphoreType.DMA
    results = pl.pallas_call(
        functools.partial(step_kernel, ntp, ndp),
        out_shape=(
            pltpu.VMEM(tokens.shape, BF16),
            pltpu.VMEM(cell.shape, F32),
            pltpu.VMEM(normer.shape, F32),
            pltpu.VMEM(stab.shape, F32),
        ),
        in_specs=[hbm] * 13,
        out_specs=(vmem,) * 4,
        scratch_shapes=[
            pltpu.VMEM((blocks, 4, width, inner), BF16),
            pltpu.VMEM((blocks, all_heads, width), BF16),
            pltpu.VMEM((blocks, all_heads, width), BF16),
            pltpu.VMEM(proj.shape, BF16),
            pltpu.VMEM((seqs, inner), F32),
            pltpu.VMEM((seqs, inner), F32),
            pltpu.VMEM((seqs, lanes), F32),
            dma,
            dma((4,)),
            pltpu.VMEM(norm_gain.shape, F32),
            pltpu.VMEM(head_gain.shape, F32),
            pltpu.VMEM(normer.shape, F32),
            pltpu.VMEM(stab.shape, F32),
            pltpu.VMEM((2, seqs * dh, heads * dh), BF16),
            pltpu.VMEM((blocks, batch, width), BF16),
            pltpu.VMEM((batch, width), BF16),
            pltpu.VMEM((blocks, 4, batch, inner), F32),
            pltpu.VMEM((blocks, gate_rows, batch), F32),
            pltpu.VMEM((blocks, ndp - 1, gate_rows, batch), F32),
            pltpu.VMEM((batch, gate_rows), F32),
            pltpu.VMEM((blocks, 4, ring, seqs, inner), F32),
            pltpu.VMEM((blocks, 4, more, seqs, inner), F32),
            pltpu.VMEM((blocks, 4, more, seqs, inner), F32),
            pltpu.VMEM((blocks, batch, inner), BF16),
            pltpu.VMEM((batch, width), F32),
            pltpu.VMEM((blocks, batch, width), BF16),
            pltpu.VMEM((blocks, ntp - 1, rows, width), BF16),
            dma((blocks, 7)),
            dma((blocks,)),
            dma((blocks, ntp - 1)),
            dma((blocks, ntp - 1)),
            dma((blocks, 4, ring)),
            dma((blocks, 4, ring)),
            dma((blocks, 4, more)),
            dma((blocks, 4, more)),
            dma((blocks, ndp - 1)),
            dma((blocks, ndp - 1)),
            dma((blocks, ndp - 1)),
            dma((blocks, ndp - 1)),
            dma((blocks, ntp - 1)),
            dma((blocks, ntp - 1)),
        ],
        compiler_params=pltpu.CompilerParams(
            collective_id=0, has_side_effects=True, vmem_limit_bytes=40 << 20
        ),
    )(
        *[
            pltpu.with_memory_space_constraint(a, pltpu.HBM)
            for a in (
                tokens, wq, wk, wv, wo, wig, wfg, norm_gain, head_gain, proj, cell, normer, stab
            )
        ]
    )

    shapes = tuple(jax.ShapeDtypeStruct(a.shape, a.dtype) for a in results)
    rows_out, cell_out, normer_out, stab_out = pl.pallas_call(
        store_kernel,
        out_shape=shapes,
        in_specs=[vmem] * 4,
        out_specs=(hbm,) * 4,
        scratch_shapes=[dma((blocks, math.gcd(seqs, 8))), dma((3,))],
        compiler_params=pltpu.CompilerParams(vmem_limit_bytes=1 << 20),
    )(*results)
    return rows_out, cell_out, normer_out, jnp.swapaxes(stab_out, 1, 2)


def solution(mesh):
    return jax.shard_map(
        functools.partial(per_device, mesh.shape["tp"], mesh.shape["dp"]),
        mesh=mesh,
        in_specs=(
            P("tp", "dp"),
            P(None, "dp", "tp"),
            P(None, "dp", "tp"),
            P(None, "dp", "tp"),
            P(None, "dp", "tp"),
            P(),
            P(),
            P(None, "dp"),
            P(None, "tp"),
            P(None, "tp", "dp"),
            P(None, "dp", "tp", None, None),
            P(None, "dp", "tp", None),
            P(None, "dp", "tp"),
        ),
        out_specs=(
            P("tp", "dp"),
            P(None, "dp", "tp", None, None),
            P(None, "dp", "tp", None),
            P(None, "dp", "tp"),
        ),
        check_vma=False,
    )
```

```python
import functools
import math

import jax
import jax.numpy as jnp
from jax import lax
from jax.experimental import pallas as pl
from jax.experimental.pallas import tpu as pltpu
from jax.sharding import PartitionSpec as P

EPSILON = 1e-06
F32 = jnp.float32
BF16 = jnp.bfloat16
MESH = pl.DeviceIdType.MESH


def split_axis(size):
    inner = max(f for f in range(1, math.isqrt(size) + 1) if size % f == 0)
    return size // inner, inner


def row_block(index, rows):
    return pl.ds(pl.multiple_of(index * rows, rows), rows)


def gate_dot(scaled, weight):
    return lax.dot_general(
        scaled, weight, (((1,), (1,)), ((), ())), preferred_element_type=F32
    )


def line_order(pos, size):
    low = jnp.minimum(pos, size - 1 - pos)
    order = []
    for k in range(1, size):
        step = (k + 1) // 2
        near = pos + (step if k % 2 == 0 else -step)
        far = jnp.where(2 * pos < size - 1, pos + k - low, pos - k + low)
        order.append(jnp.where(k <= 2 * low, near, far))
    return order


def step_kernel(
    ntp,
    ndp,
    tokens,
    wq,
    wk,
    wv,
    wo,
    wig,
    wfg,
    norm_gain,
    head_gain,
    proj,
    cell,
    normer,
    stab,
    final_out,
    cell_buf,
    normer_out,
    stab_out,
    w_buf,
    ig_buf,
    fg_buf,
    proj_buf,
    written_buf,
    key_buf,
    keep_buf,
    tok_sem,
    small_sem,
    gain_buf,
    head_buf,
    normer_buf,
    stab_buf,
    split_buf,
    current,
    scaled_buf,
    partial,
    gates,
    gate_recv,
    gate_cols,
    pair_recv,
    pair_sum,
    proj_recv,
    gated_all,
    out_part,
    out_stage,
    out_recv,
    load_sem,
    cell_sem,
    ag_send,
    ag_recv,
    pr_send,
    pr_recv,
    rs_send,
    rs_recv,
    gt_send,
    gt_recv,
    gg_send,
    gg_recv,
    os_send,
    os_recv,
):
    blocks = wq.shape[0]
    width, inner = wq.shape[1], wq.shape[2]
    all_heads = wig.shape[1]
    seqs, heads, dh = cell.shape[1], cell.shape[2], cell.shape[3]
    rows = tokens.shape[0]
    batch = rows * ntp
    t = lax.axis_index("tp")
    d = lax.axis_index("dp")
    outer, side = split_axis(ntp)
    z = t // side
    x = lax.rem(t, side)
    z_order = line_order(z, outer)

    pair = 2 if ndp % 2 == 0 else 1
    ring = ndp // pair
    y = d // pair
    core = lax.rem(d, pair)
    own = row_block(d, seqs)
    mine = row_block(t, rows)

    tok_load = pltpu.make_async_copy(tokens, current.at[0, mine], tok_sem)
    tok_load.start()
    barrier = pltpu.get_barrier_semaphore()
    for k in range(1, ntp):
        pl.semaphore_signal(
            barrier, inc=1, device_id={"tp": lax.rem(t + k, ntp)}, device_id_type=MESH
        )
    for k in range(1, ndp):
        pl.semaphore_signal(
            barrier, inc=1, device_id={"dp": lax.rem(d + k, ndp)}, device_id_type=MESH
        )
    small = [
        pltpu.make_async_copy(src, dst, small_sem.at[i])
        for i, (src, dst) in enumerate(
            (
                (norm_gain, gain_buf),
                (head_gain, head_buf),
                (normer, normer_buf),
                (stab, stab_buf),
            )
        )
    ]
    loads = []
    for b in range(blocks):
        one = [
            pltpu.make_async_copy(w.at[b], w_buf.at[b, i], load_sem.at[b, i])
            for i, w in enumerate((wq, wk, wv, wo))
        ]
        one.append(
            pltpu.make_async_copy(
                wig.at[b, :, row_block(d, width)], ig_buf.at[b], load_sem.at[b, 4]
            )
        )
        one.append(
            pltpu.make_async_copy(
                wfg.at[b, :, row_block(d, width)], fg_buf.at[b], load_sem.at[b, 5]
            )
        )
        one.append(pltpu.make_async_copy(proj.at[b], proj_buf.at[b], load_sem.at[b, 6]))
        loads.append(one)
    cell_loads = [
        pltpu.make_async_copy(cell.at[b], cell_buf.at[b], cell_sem.at[b]) for b in range(blocks)
    ]
    tok_load.wait()
    for c in small:
        c.start()
    for c in loads[0]:
        c.start()
    cell_loads[0].start()
    pl.semaphore_wait(barrier, ntp - 1 + ndp - 1)

    def split_cells(b):
        cell_loads[b].wait()

        def one(i, _):
            for h in range(heads):
                whole = cell_buf[b, i, h]
                high = whole.astype(BF16)
                here, lanes = row_block(i, dh), slice(h * dh, (h + 1) * dh)
                split_buf[0, here, lanes] = high
                split_buf[1, here, lanes] = (whole - high.astype(F32)).astype(BF16)
            return 0

        lax.fori_loop(0, seqs, one, 0)

    eight = math.gcd(seqs, 8)

    def update_cells(b):
        def one(c, _):
            here = row_block(c, eight)
            keep = keep_buf[here, :]
            for h in range(heads):
                lanes = slice(h * dh, (h + 1) * dh)
                across = jnp.transpose(written_buf[here, lanes])
                keys = key_buf[here, lanes]
                for j in range(eight):
                    cell_buf[b, c * eight + j, h] = (
                        keep[j : j + 1, h : h + 1] * cell_buf[b, c * eight + j, h]
                        + across[:, j : j + 1] * keys[j : j + 1, :]
                    )
            return 0

        lax.fori_loop(0, seqs // eight, one, 0)

    def ag_copy(b, block, slot, dest):
        here = row_block(block, rows)
        return pltpu.make_async_remote_copy(
            src_ref=current.at[b, here],
            dst_ref=current.at[b, here],
            send_sem=ag_send.at[b, slot],
            recv_sem=ag_recv.at[b, slot],
            device_id={"tp": dest},
            device_id_type=MESH,
        )

    def gather_start(b):
        sent = []
        for zd in reversed(z_order):
            sent.append(ag_copy(b, t, lax.rem(zd - z + outer, outer) - 1, zd * side + x))
        for j in range(1, side):
            dest = z * side + lax.rem(x + j, side)
            sent.append(ag_copy(b, t, outer - 1 + (j - 1) * outer, dest))
        for c in sent:
            c.start()
        return sent

    def gather_finish(b, sent):
        for zs in z_order:
            gap = lax.rem(z - zs + outer, outer)
            block = zs * side + x
            ag_copy(b, block, gap - 1, block).wait_recv()
            for j in range(1, side):
                dest = z * side + lax.rem(x + j, side)
                copy = ag_copy(b, block, outer - 1 + (j - 1) * outer + gap, dest)
                copy.start()
                sent.append(copy)
        for j in range(1, side):
            xs = lax.rem(x - j + side, side)
            from_x = z * side + xs
            ag_copy(b, from_x, outer - 1 + (j - 1) * outer, from_x).wait_recv()
            for zs in z_order:
                gap = lax.rem(z - zs + outer, outer)
                slot = outer - 1 + (j - 1) * outer + gap
                ag_copy(b, zs * side + xs, slot, from_x).wait_recv()
        return sent

    gather = gather_start(0)
    for b in range(blocks):
        sends = gather_finish(b, gather)
        if b == 0:
            for c in small:
                c.wait()
            for later in range(1, blocks):
                for c in loads[later]:
                    c.start()
                cell_loads[later].start()
        as_float = current[b].astype(F32)
        scaled_buf[...] = (as_float * gain_buf[b : b + 1, :]).astype(BF16)

        def dp_send(src, dst, send_sem, recv_sem, dest):
            copy = pltpu.make_async_remote_copy(
                src_ref=src,
                dst_ref=dst,
                send_sem=send_sem,
                recv_sem=recv_sem,
                device_id={"dp": dest},
                device_id_type=MESH,
            )
            copy.start()
            sends.append(copy)
            return copy

        mate = y * pair + (pair - 1 - core)
        for i in range(4):
            loads[b][i].wait()
        for i in range(4):
            partial[b, i] = jnp.dot(scaled_buf[...], w_buf[b, i], preferred_element_type=F32)
        paired = []
        for i in range(4):
            one = {}
            if pair == 2:
                for k in range(ring):
                    slot = (k + 1) % ring
                    block = row_block(lax.rem(y + slot, ring) * pair + 1 - core, seqs)
                    one[slot] = dp_send(
                        partial.at[b, i, block],
                        pair_recv.at[b, i, slot],
                        pr_send.at[b, i, slot],
                        pr_recv.at[b, i, slot],
                        mate,
                    )
            paired.append(one)

        for c in loads[b][4:]:
            c.wait()
        gate_copies = [
            pltpu.make_async_remote_copy(
                src_ref=gates.at[b],
                dst_ref=gate_recv.at[b, k - 1],
                send_sem=gt_send.at[b, k - 1],
                recv_sem=gt_recv.at[b, k - 1],
                device_id={"dp": lax.rem(d + k, ndp)},
                device_id_type=MESH,
            )
            for k in sorted(range(1, ndp), key=lambda k: -min(k, ndp - k))
        ]
        sends.extend(gate_copies)

        def send_gates():
            square = current[b].astype(F32) * current[b].astype(F32)
            high = square.astype(BF16)
            low = (square - high.astype(F32)).astype(BF16)
            ones = jnp.ones((16, width), BF16)
            squares = gate_dot(ones, high) + gate_dot(ones, low)
            igates = gate_dot(ig_buf[b], scaled_buf[...])
            fgates = gate_dot(fg_buf[b], scaled_buf[...])
            head_row = lax.broadcasted_iota(jnp.int32, (all_heads, batch), 0)
            lines = []
            for source in (igates, fgates):
                for h in range(heads):
                    hit = head_row == t * heads + h
                    lines.append(jnp.sum(jnp.where(hit, source, 0.0), axis=0, keepdims=True))
            lines.append(squares[0:1])
            line = lax.broadcasted_iota(jnp.int32, gates.shape[1:], 0)
            packed = jnp.zeros(gates.shape[1:], F32)
            for r, value in enumerate(lines):
                packed = jnp.where(line == r, jnp.broadcast_to(value, packed.shape), packed)
            gates[b] = packed
            for c in gate_copies:
                c.start()

        def reduce_pair(i):
            one = []
            for slot in range(1, ring):
                dest = lax.rem(y + slot, ring) * pair + core
                summed = partial[b, i, row_block(dest, seqs), :]
                if pair == 2:
                    paired[i][slot].wait_recv()
                    summed = summed + pair_recv[b, i, slot]
                pair_sum[b, i, slot - 1] = summed
                one.append(
                    dp_send(
                        pair_sum.at[b, i, slot - 1],
                        proj_recv.at[b, i, slot - 1],
                        rs_send.at[b, i, slot - 1],
                        rs_recv.at[b, i, slot - 1],
                        dest,
                    )
                )
            return one

        ahead = core == pair - 1 if pair == 2 else d < 0
        pl.when(ahead)(send_gates)
        arriving = [reduce_pair(0)]
        pl.when(jnp.logical_not(ahead))(send_gates)
        arriving += [reduce_pair(i) for i in range(1, 4)]
        if b == 0:
            split_cells(0)

        def total(i):
            value = partial[b, i, own, :]
            if pair == 2:
                value = value + pair_recv[b, i, 0]
            for k in range(ring - 1):
                value = value + proj_recv[b, i, k]
            return value

        def arrived(i):
            if pair == 2:
                paired[i][0].wait_recv()
            for k in range(ring - 1):
                arriving[i][k].wait_recv()

        arrived(0)
        for c in gate_copies:
            c.wait_recv()
        gate_sum = gates[b]
        for k in range(ndp - 1):
            gate_sum = gate_sum + gate_recv[b, k]
        gate_cols[...] = jnp.transpose(gate_sum)
        pre = gate_cols[own, :]
        inv_rms = lax.rsqrt(pre[:, 2 * heads : 2 * heads + 1] / (width * ndp) + EPSILON)
        pre = pre * inv_rms
        diag = lax.broadcasted_iota(jnp.int32, (seqs, seqs), 0) == (
            lax.broadcasted_iota(jnp.int32, (seqs, seqs), 1)
        )
        lane = lax.broadcasted_iota(jnp.int32, keep_buf.shape, 1)
        aux = jnp.zeros(keep_buf.shape, F32)
        keeps, writes = [], []
        for h in range(heads):
            igate, fpre = pre[:, h : h + 1], pre[:, heads + h : heads + h + 1]
            lf = jnp.minimum(fpre, 0.0) - jnp.log1p(jnp.exp(-jnp.abs(fpre)))
            stab_row = jnp.broadcast_to(stab_buf[b, h : h + 1, :], (seqs, seqs))
            m0 = jnp.sum(jnp.where(diag, stab_row, 0.0), axis=1, keepdims=True)
            carried = lf + m0
            m1 = jnp.maximum(carried, igate)
            stab_out[b, h : h + 1, :] = jnp.sum(jnp.where(diag, m1, 0.0), axis=0, keepdims=True)
            keeps.append(jnp.exp(carried - m1))
            writes.append(jnp.exp(igate - m1))
            aux = jnp.where(lane == h, keeps[h], aux)
        keep_buf[...] = aux

        raw = total(0)
        wide = -(-2 * heads * seqs // 128) * 128
        column = lax.rem(lax.broadcasted_iota(jnp.int32, (dh, wide), 1), seqs)
        terms = []
        for h in range(heads):
            high = raw[:, h * dh : (h + 1) * dh].astype(BF16)
            low = (raw[:, h * dh : (h + 1) * dh] - high.astype(F32)).astype(BF16)
            for part in (high, low):
                blank = jnp.zeros(part.shape, BF16)
                terms.append(jnp.concatenate([part if g == h else blank for g in range(heads)], 1))
        if wide > 2 * heads * seqs:
            terms.append(jnp.zeros((wide - 2 * heads * seqs, heads * dh), BF16))
        rhs = jnp.concatenate(terms, 0)
        acc = jnp.zeros((dh, wide), F32)
        for c in range(seqs // eight):
            here = slice(c * eight * dh, (c + 1) * eight * dh)
            prod = gate_dot(split_buf[0, here, :], rhs) + gate_dot(split_buf[1, here, :], rhs)
            for j in range(eight):
                acc = jnp.where(column == c * eight + j, prod[j * dh : (j + 1) * dh], acc)
        turned = jnp.transpose(acc)
        reads = [
            (
                turned[2 * h * seqs : (2 * h + 1) * seqs]
                + turned[(2 * h + 1) * seqs : (2 * h + 2) * seqs]
            )
            * inv_rms
            for h in range(heads)
        ]
        for i in range(1, 4):
            arrived(i)
        query = raw * inv_rms
        key = total(1) * inv_rms * (dh ** (-0.5))
        key_buf[...] = key
        dots, normers = [], []
        for h in range(heads):
            lanes = slice(h * dh, (h + 1) * dh)
            qh, kh = query[:, lanes], key[:, lanes]
            n1 = keeps[h] * normer_buf[b, :, h, :] + writes[h] * kh
            normer_out[b, :, h, :] = n1
            dots.append(jnp.sum(kh * qh, axis=1, keepdims=True))
            normers.append(jnp.sum(n1 * qh, axis=1, keepdims=True))
        value = total(2) * inv_rms
        normed = []
        for h in range(heads):
            lanes = slice(h * dh, (h + 1) * dh)
            written = writes[h] * value[:, lanes]
            written_buf[:, lanes] = written
            numer = keeps[h] * reads[h] + written * dots[h]
            readout = numer / jnp.maximum(jnp.abs(normers[h]), 1.0)
            one = readout * lax.rsqrt(jnp.mean(readout * readout, axis=1, keepdims=True) + EPSILON)
            normed.append(one * head_buf[b : b + 1, lanes])
        outgate = total(3) * inv_rms
        for h in range(heads):
            lanes = slice(h * dh, (h + 1) * dh)
            gate = 1.0 / (1.0 + jnp.exp(-outgate[:, lanes]))
            gated_all[b, own, lanes] = (gate * normed[h]).astype(BF16)

        spread = []
        for k in sorted(range(1, ndp), key=lambda k: -min(k, ndp - k)):
            spread.append(
                dp_send(
                    gated_all.at[b, own],
                    gated_all.at[b, own],
                    gg_send.at[b, k - 1],
                    gg_recv.at[b, k - 1],
                    lax.rem(d + k, ndp),
                )
            )
        for c in spread:
            c.wait_recv()
        part = jnp.dot(gated_all[b], proj_buf[b], preferred_element_type=F32)
        out_stage[b] = part.astype(BF16)
        out_part[...] = part
        outs = []
        for zd in list(reversed(z_order)) + [z]:
            for xd in range(1 if zd is z else 0, side):
                dest = zd * side + lax.rem(x + xd, side)
                slot = lax.rem(dest - t + ntp, ntp) - 1
                copy = pltpu.make_async_remote_copy(
                    src_ref=out_stage.at[b, row_block(dest, rows)],
                    dst_ref=out_recv.at[b, slot],
                    send_sem=os_send.at[b, slot],
                    recv_sem=os_recv.at[b, slot],
                    device_id={"tp": dest},
                    device_id_type=MESH,
                )
                copy.start()
                outs.append(copy)
        update_cells(b)
        if b + 1 < blocks:
            split_cells(b + 1)
        for c in outs:
            c.wait_recv()
        summed = out_part[mine, :]
        for k in range(ntp - 1):
            summed = summed + out_recv[b, k].astype(F32)
        if b + 1 < blocks:
            current[b + 1, mine, :] = summed.astype(BF16)
            gather = gather_start(b + 1)
        else:
            final_out[...] = summed.astype(BF16)
        for c in sends + outs:
            c.wait_send()


def store_kernel(rows, cell, normer, stab, rows_out, cell_out, normer_out, stab_out, cell_sem, sems):
    blocks, seqs = cell.shape[0], cell.shape[1]
    parts = cell_sem.shape[1]
    step = seqs // parts
    copies = [
        pltpu.make_async_copy(
            cell.at[b, i * step : (i + 1) * step],
            cell_out.at[b, i * step : (i + 1) * step],
            cell_sem.at[b, i],
        )
        for b in range(blocks)
        for i in range(parts)
    ]
    for i, (src, dst) in enumerate(((rows, rows_out), (normer, normer_out), (stab, stab_out))):
        copies.append(pltpu.make_async_copy(src, dst, sems.at[i]))
    for c in copies:
        c.start()
    for c in copies:
        c.wait()


def per_device(ntp, ndp, *args):
    (tokens, wq, wk, wv, wo, wig, wfg, norm_gain, head_gain, proj, cell, normer, stab) = args
    blocks, width, inner = wq.shape
    all_heads = wig.shape[2]
    seqs, heads, dh = cell.shape[1], cell.shape[2], cell.shape[3]
    rows = tokens.shape[0]
    pair = 2 if ndp % 2 == 0 else 1
    ring = ndp // pair
    more = max(ring - 1, 1)
    wig, wfg, stab = (jnp.swapaxes(a, 1, 2) for a in (wig, wfg, stab))
    batch = rows * ntp
    lanes = -(-heads // 128) * 128
    gate_rows = -(-(2 * heads + 1) // 8) * 8
    vmem = pl.BlockSpec(memory_space=pltpu.VMEM)
    hbm = pl.BlockSpec(memory_space=pltpu.HBM)
    dma = pltpu.SemaphoreType.DMA
    results = pl.pallas_call(
        functools.partial(step_kernel, ntp, ndp),
        out_shape=(
            pltpu.VMEM(tokens.shape, BF16),
            pltpu.VMEM(cell.shape, F32),
            pltpu.VMEM(normer.shape, F32),
            pltpu.VMEM(stab.shape, F32),
        ),
        in_specs=[hbm] * 13,
        out_specs=(vmem,) * 4,
        scratch_shapes=[
            pltpu.VMEM((blocks, 4, width, inner), BF16),
            pltpu.VMEM((blocks, all_heads, width), BF16),
            pltpu.VMEM((blocks, all_heads, width), BF16),
            pltpu.VMEM(proj.shape, BF16),
            pltpu.VMEM((seqs, inner), F32),
            pltpu.VMEM((seqs, inner), F32),
            pltpu.VMEM((seqs, lanes), F32),
            dma,
            dma((4,)),
            pltpu.VMEM(norm_gain.shape, F32),
            pltpu.VMEM(head_gain.shape, F32),
            pltpu.VMEM(normer.shape, F32),
            pltpu.VMEM(stab.shape, F32),
            pltpu.VMEM((2, seqs * dh, heads * dh), BF16),
            pltpu.VMEM((blocks, batch, width), BF16),
            pltpu.VMEM((batch, width), BF16),
            pltpu.VMEM((blocks, 4, batch, inner), F32),
            pltpu.VMEM((blocks, gate_rows, batch), F32),
            pltpu.VMEM((blocks, ndp - 1, gate_rows, batch), F32),
            pltpu.VMEM((batch, gate_rows), F32),
            pltpu.VMEM((blocks, 4, ring, seqs, inner), F32),
            pltpu.VMEM((blocks, 4, more, seqs, inner), F32),
            pltpu.VMEM((blocks, 4, more, seqs, inner), F32),
            pltpu.VMEM((blocks, batch, inner), BF16),
            pltpu.VMEM((batch, width), F32),
            pltpu.VMEM((blocks, batch, width), BF16),
            pltpu.VMEM((blocks, ntp - 1, rows, width), BF16),
            dma((blocks, 7)),
            dma((blocks,)),
            dma((blocks, ntp - 1)),
            dma((blocks, ntp - 1)),
            dma((blocks, 4, ring)),
            dma((blocks, 4, ring)),
            dma((blocks, 4, more)),
            dma((blocks, 4, more)),
            dma((blocks, ndp - 1)),
            dma((blocks, ndp - 1)),
            dma((blocks, ndp - 1)),
            dma((blocks, ndp - 1)),
            dma((blocks, ntp - 1)),
            dma((blocks, ntp - 1)),
        ],
        compiler_params=pltpu.CompilerParams(
            collective_id=0, has_side_effects=True, vmem_limit_bytes=40 << 20
        ),
    )(
        *[
            pltpu.with_memory_space_constraint(a, pltpu.HBM)
            for a in (
                tokens, wq, wk, wv, wo, wig, wfg, norm_gain, head_gain, proj, cell, normer, stab
            )
        ]
    )

    shapes = tuple(jax.ShapeDtypeStruct(a.shape, a.dtype) for a in results)
    rows_out, cell_out, normer_out, stab_out = pl.pallas_call(
        store_kernel,
        out_shape=shapes,
        in_specs=[vmem] * 4,
        out_specs=(hbm,) * 4,
        scratch_shapes=[dma((blocks, math.gcd(seqs, 8))), dma((3,))],
        compiler_params=pltpu.CompilerParams(vmem_limit_bytes=1 << 20),
    )(*results)
    return rows_out, cell_out, normer_out, jnp.swapaxes(stab_out, 1, 2)


def solution(mesh):
    return jax.shard_map(
        functools.partial(per_device, mesh.shape["tp"], mesh.shape["dp"]),
        mesh=mesh,
        in_specs=(
            P("tp", "dp"),
            P(None, "dp", "tp"),
            P(None, "dp", "tp"),
            P(None, "dp", "tp"),
            P(None, "dp", "tp"),
            P(),
            P(),
            P(None, "dp"),
            P(None, "tp"),
            P(None, "tp", "dp"),
            P(None, "dp", "tp", None, None),
            P(None, "dp", "tp", None),
            P(None, "dp", "tp"),
        ),
        out_specs=(
            P("tp", "dp"),
            P(None, "dp", "tp", None, None),
            P(None, "dp", "tp", None),
            P(None, "dp", "tp"),
        ),
        check_vma=False,
    )
```

```python
import functools
import math

import jax
import jax.numpy as jnp
from jax import lax
from jax.experimental import pallas as pl
from jax.experimental.pallas import tpu as pltpu
from jax.sharding import PartitionSpec as P

EPSILON = 1e-06
F32 = jnp.float32
BF16 = jnp.bfloat16
MESH = pl.DeviceIdType.MESH


def split_axis(size):
    inner = max(f for f in range(1, math.isqrt(size) + 1) if size % f == 0)
    return size // inner, inner


def row_block(index, rows):
    return pl.ds(pl.multiple_of(index * rows, rows), rows)


def gate_dot(scaled, weight):
    return lax.dot_general(
        scaled, weight, (((1,), (1,)), ((), ())), preferred_element_type=F32
    )


def line_order(pos, size):
    low = jnp.minimum(pos, size - 1 - pos)
    order = []
    for k in range(1, size):
        step = (k + 1) // 2
        near = pos + (step if k % 2 == 0 else -step)
        far = jnp.where(2 * pos < size - 1, pos + k - low, pos - k + low)
        order.append(jnp.where(k <= 2 * low, near, far))
    return order


def step_kernel(
    ntp,
    ndp,
    tokens,
    wq,
    wk,
    wv,
    wo,
    wig,
    wfg,
    norm_gain,
    head_gain,
    proj,
    cell,
    normer,
    stab,
    final_out,
    cell_buf,
    normer_out,
    stab_out,
    w_buf,
    ig_buf,
    fg_buf,
    proj_buf,
    written_buf,
    key_buf,
    keep_buf,
    tok_sem,
    small_sem,
    gain_buf,
    head_buf,
    normer_buf,
    stab_buf,
    split_buf,
    current,
    mixed,
    scaled_buf,
    partial,
    mixed_partial,
    gates,
    gate_recv,
    gate_cols,
    pair_recv,
    pair_sum,
    proj_recv,
    pair_narrow,
    narrow_recv,
    gated_all,
    out_part,
    out_stage,
    out_recv,
    mix_stage,
    mix_recv,
    load_sem,
    cell_sem,
    ag_send,
    ag_recv,
    pr_send,
    pr_recv,
    rs_send,
    rs_recv,
    gt_send,
    gt_recv,
    gg_send,
    gg_recv,
    os_send,
    os_recv,
    ms_send,
    ms_recv,
):
    blocks = wq.shape[0]
    width, inner = wq.shape[1], wq.shape[2]
    all_heads = wig.shape[1]
    seqs, heads, dh = cell.shape[1], cell.shape[2], cell.shape[3]
    rows = tokens.shape[0]
    batch = rows * ntp
    t = lax.axis_index("tp")
    d = lax.axis_index("dp")
    outer, side = split_axis(ntp)
    z = t // side
    x = lax.rem(t, side)
    z_order = line_order(z, outer)

    pair = 2 if ndp % 2 == 0 else 1
    ring = ndp // pair
    y = d // pair
    core = lax.rem(d, pair)
    own = row_block(d, seqs)
    mine = row_block(t, rows)
    few, half = seqs // outer, width // side

    tok_load = pltpu.make_async_copy(tokens, current.at[mine], tok_sem)
    tok_load.start()
    barrier = pltpu.get_barrier_semaphore()
    for k in range(1, ntp):
        pl.semaphore_signal(
            barrier, inc=1, device_id={"tp": lax.rem(t + k, ntp)}, device_id_type=MESH
        )
    for k in range(1, ndp):
        pl.semaphore_signal(
            barrier, inc=1, device_id={"dp": lax.rem(d + k, ndp)}, device_id_type=MESH
        )
    small = [
        pltpu.make_async_copy(src, dst, small_sem.at[i])
        for i, (src, dst) in enumerate(
            (
                (norm_gain, gain_buf),
                (head_gain, head_buf),
                (normer, normer_buf),
                (stab, stab_buf),
            )
        )
    ]
    loads = []
    for b in range(blocks):
        one = [
            pltpu.make_async_copy(w.at[b], w_buf.at[b, i], load_sem.at[b, i])
            for i, w in enumerate((wq, wk, wv, wo))
        ]
        one.append(
            pltpu.make_async_copy(
                wig.at[b, :, row_block(d, width)], ig_buf.at[b], load_sem.at[b, 4]
            )
        )
        one.append(
            pltpu.make_async_copy(
                wfg.at[b, :, row_block(d, width)], fg_buf.at[b], load_sem.at[b, 5]
            )
        )
        one.append(pltpu.make_async_copy(proj.at[b], proj_buf.at[b], load_sem.at[b, 6]))
        loads.append(one)
    cell_loads = [
        pltpu.make_async_copy(cell.at[b], cell_buf.at[b], cell_sem.at[b]) for b in range(blocks)
    ]
    tok_load.wait()
    for c in small:
        c.start()
    for c in loads[0]:
        c.start()
    cell_loads[0].start()
    pl.semaphore_wait(barrier, ntp - 1 + ndp - 1)

    def split_cells(b):
        cell_loads[b].wait()

        def one(i, _):
            for h in range(heads):
                whole = cell_buf[b, i, h]
                high = whole.astype(BF16)
                here, lanes = row_block(i, dh), slice(h * dh, (h + 1) * dh)
                split_buf[0, here, lanes] = high
                if b + 1 < blocks:
                    split_buf[1, here, lanes] = (whole - high.astype(F32)).astype(BF16)
            return 0

        lax.fori_loop(0, seqs, one, 0)

    eight = math.gcd(seqs, 8)

    def update_cells(b):
        def one(c, _):
            here = row_block(c, eight)
            keep = keep_buf[here, :]
            for h in range(heads):
                lanes = slice(h * dh, (h + 1) * dh)
                across = jnp.transpose(written_buf[here, lanes])
                keys = key_buf[here, lanes]
                for j in range(eight):
                    cell_buf[b, c * eight + j, h] = (
                        keep[j : j + 1, h : h + 1] * cell_buf[b, c * eight + j, h]
                        + across[:, j : j + 1] * keys[j : j + 1, :]
                    )
            return 0

        lax.fori_loop(0, seqs // eight, one, 0)

    def ag_copy(b, block, slot, dest):
        if b == 0:
            here = current.at[row_block(block, rows)]
        else:
            here = mixed.at[b - 1, lax.rem(block, side), block // side]
        return pltpu.make_async_remote_copy(
            src_ref=here,
            dst_ref=here,
            send_sem=ag_send.at[b, slot],
            recv_sem=ag_recv.at[b, slot],
            device_id={"tp": dest},
            device_id_type=MESH,
        )

    def gather_start(b):
        sent = []
        for zd in reversed(z_order):
            sent.append(ag_copy(b, t, lax.rem(zd - z + outer, outer) - 1, zd * side + x))
        for j in range(1, side):
            dest = z * side + lax.rem(x + j, side)
            sent.append(ag_copy(b, t, outer - 1 + (j - 1) * outer, dest))
        for c in sent:
            c.start()
        return sent

    def gather_finish(b, sent):
        for zs in z_order:
            gap = lax.rem(z - zs + outer, outer)
            block = zs * side + x
            ag_copy(b, block, gap - 1, block).wait_recv()
            for j in range(1, side):
                dest = z * side + lax.rem(x + j, side)
                copy = ag_copy(b, block, outer - 1 + (j - 1) * outer + gap, dest)
                copy.start()
                sent.append(copy)
        for j in range(1, side):
            xs = lax.rem(x - j + side, side)
            from_x = z * side + xs
            ag_copy(b, from_x, outer - 1 + (j - 1) * outer, from_x).wait_recv()
            for zs in z_order:
                gap = lax.rem(z - zs + outer, outer)
                slot = outer - 1 + (j - 1) * outer + gap
                ag_copy(b, zs * side + xs, slot, from_x).wait_recv()
        return sent

    gather = gather_start(0)
    for b in range(blocks):
        sends = gather_finish(b, gather)
        if b == 0:
            for c in small:
                c.wait()
            for later in range(1, blocks):
                for c in loads[later]:
                    c.start()
                cell_loads[later].start()
        def load_current():
            if b == 0:
                return current[...].astype(F32)
            parts = [mixed[b - 1, i].reshape(batch, half).astype(F32) for i in range(side)]
            return jnp.concatenate(parts, 1)

        def seq_rows(i, block):
            return partial.at[i, block] if b == 0 else mixed_partial.at[b - 1, i, :, block]

        def narrow(i):
            return b + 1 == blocks and i >= 2

        scaled_buf[...] = (load_current() * gain_buf[b : b + 1, :]).astype(BF16)

        def dp_send(src, dst, send_sem, recv_sem, dest):
            copy = pltpu.make_async_remote_copy(
                src_ref=src,
                dst_ref=dst,
                send_sem=send_sem,
                recv_sem=recv_sem,
                device_id={"dp": dest},
                device_id_type=MESH,
            )
            copy.start()
            sends.append(copy)
            return copy

        mate = y * pair + (pair - 1 - core)
        for i in range(4):
            loads[b][i].wait()
        for i in range(4):
            product = jnp.dot(scaled_buf[...], w_buf[b, i], preferred_element_type=F32)
            if b == 0:
                partial[i] = product.reshape(ndp, outer, few, inner)
            else:
                mixed_partial[b - 1, i] = product.reshape(outer, ndp, few, inner)
        paired = []
        for i in range(4):
            one = {}
            if pair == 2:
                for k in range(ring):
                    slot = (k + 1) % ring
                    block = lax.rem(y + slot, ring) * pair + 1 - core
                    one[slot] = dp_send(
                        seq_rows(i, block),
                        pair_recv.at[b, i, slot],
                        pr_send.at[b, i, slot],
                        pr_recv.at[b, i, slot],
                        mate,
                    )
            paired.append(one)

        for c in loads[b][4:]:
            c.wait()
        gate_copies = [
            pltpu.make_async_remote_copy(
                src_ref=gates.at[b],
                dst_ref=gate_recv.at[b, k - 1],
                send_sem=gt_send.at[b, k - 1],
                recv_sem=gt_recv.at[b, k - 1],
                device_id={"dp": lax.rem(d + k, ndp)},
                device_id_type=MESH,
            )
            for k in sorted(range(1, ndp), key=lambda k: -min(k, ndp - k))
        ]
        sends.extend(gate_copies)

        def send_gates():
            plain = load_current()
            square = plain * plain
            high = square.astype(BF16)
            low = (square - high.astype(F32)).astype(BF16)
            ones = jnp.ones((16, width), BF16)
            squares = gate_dot(ones, high) + gate_dot(ones, low)
            igates = gate_dot(ig_buf[b], scaled_buf[...])
            fgates = gate_dot(fg_buf[b], scaled_buf[...])
            head_row = lax.broadcasted_iota(jnp.int32, (all_heads, batch), 0)
            lines = []
            for source in (igates, fgates):
                for h in range(heads):
                    hit = head_row == t * heads + h
                    lines.append(jnp.sum(jnp.where(hit, source, 0.0), axis=0, keepdims=True))
            lines.append(squares[0:1])
            line = lax.broadcasted_iota(jnp.int32, gates.shape[1:], 0)
            packed = jnp.zeros(gates.shape[1:], F32)
            for r, value in enumerate(lines):
                packed = jnp.where(line == r, jnp.broadcast_to(value, packed.shape), packed)
            gates[b] = packed
            for c in gate_copies:
                c.start()

        def reduce_pair(i):
            one = []
            for slot in range(1, ring):
                dest = lax.rem(y + slot, ring) * pair + core
                summed = seq_rows(i, dest)[...]
                if pair == 2:
                    paired[i][slot].wait_recv()
                    summed = summed + pair_recv[b, i, slot]
                if narrow(i):
                    src, dst = pair_narrow.at[i - 2, slot - 1], narrow_recv.at[i - 2, slot - 1]
                else:
                    src, dst = pair_sum.at[b, i, slot - 1], proj_recv.at[b, i, slot - 1]
                src[...] = summed.astype(src.dtype).reshape(src.shape)
                one.append(
                    dp_send(
                        src,
                        dst,
                        rs_send.at[b, i, slot - 1],
                        rs_recv.at[b, i, slot - 1],
                        dest,
                    )
                )
            return one

        ahead = core == pair - 1 if pair == 2 else d < 0
        pl.when(ahead)(send_gates)
        arriving = [reduce_pair(0)]
        pl.when(jnp.logical_not(ahead))(send_gates)
        arriving += [reduce_pair(i) for i in range(1, 4)]
        if b == 0:
            split_cells(0)

        def total(i):
            value = seq_rows(i, d)[...]
            if pair == 2:
                value = value + pair_recv[b, i, 0]
            value = value.reshape(seqs, inner)
            for k in range(ring - 1):
                if narrow(i):
                    value = value + narrow_recv[i - 2, k].astype(F32)
                else:
                    value = value + proj_recv[b, i, k].reshape(seqs, inner)
            return value

        def arrived(i):
            if pair == 2:
                paired[i][0].wait_recv()
            for k in range(ring - 1):
                arriving[i][k].wait_recv()

        arrived(0)
        for c in gate_copies:
            c.wait_recv()
        gate_sum = gates[b]
        for k in range(ndp - 1):
            gate_sum = gate_sum + gate_recv[b, k]
        gate_cols[...] = jnp.transpose(gate_sum)
        if b == 0:
            pre = gate_cols[own, :]
        else:
            pre = jnp.concatenate(
                [gate_cols[row_block(i * ndp + d, few), :] for i in range(outer)], 0
            )
        inv_rms = lax.rsqrt(pre[:, 2 * heads : 2 * heads + 1] / (width * ndp) + EPSILON)
        pre = pre * inv_rms
        diag = lax.broadcasted_iota(jnp.int32, (seqs, seqs), 0) == (
            lax.broadcasted_iota(jnp.int32, (seqs, seqs), 1)
        )
        lane = lax.broadcasted_iota(jnp.int32, keep_buf.shape, 1)
        aux = jnp.zeros(keep_buf.shape, F32)
        keeps, writes = [], []
        for h in range(heads):
            igate, fpre = pre[:, h : h + 1], pre[:, heads + h : heads + h + 1]
            lf = jnp.minimum(fpre, 0.0) - jnp.log1p(jnp.exp(-jnp.abs(fpre)))
            stab_row = jnp.broadcast_to(stab_buf[b, h : h + 1, :], (seqs, seqs))
            m0 = jnp.sum(jnp.where(diag, stab_row, 0.0), axis=1, keepdims=True)
            carried = lf + m0
            m1 = jnp.maximum(carried, igate)
            stab_out[b, h : h + 1, :] = jnp.sum(jnp.where(diag, m1, 0.0), axis=0, keepdims=True)
            keeps.append(jnp.exp(carried - m1))
            writes.append(jnp.exp(igate - m1))
            aux = jnp.where(lane == h, keeps[h], aux)
        keep_buf[...] = aux

        raw = total(0)
        wide = -(-2 * heads * seqs // 128) * 128
        column = lax.rem(lax.broadcasted_iota(jnp.int32, (dh, wide), 1), seqs)
        terms = []
        for h in range(heads):
            high = raw[:, h * dh : (h + 1) * dh].astype(BF16)
            low = (raw[:, h * dh : (h + 1) * dh] - high.astype(F32)).astype(BF16)
            for part in (high, low):
                blank = jnp.zeros(part.shape, BF16)
                terms.append(jnp.concatenate([part if g == h else blank for g in range(heads)], 1))
        if wide > 2 * heads * seqs:
            terms.append(jnp.zeros((wide - 2 * heads * seqs, heads * dh), BF16))
        rhs = jnp.concatenate(terms, 0)
        acc = jnp.zeros((dh, wide), F32)
        for c in range(seqs // eight):
            here = slice(c * eight * dh, (c + 1) * eight * dh)
            prod = gate_dot(split_buf[0, here, :], rhs)
            if b + 1 < blocks:
                prod = prod + gate_dot(split_buf[1, here, :], rhs)
            for j in range(eight):
                acc = jnp.where(column == c * eight + j, prod[j * dh : (j + 1) * dh], acc)
        turned = jnp.transpose(acc)
        reads = [
            (
                turned[2 * h * seqs : (2 * h + 1) * seqs]
                + turned[(2 * h + 1) * seqs : (2 * h + 2) * seqs]
            )
            * inv_rms
            for h in range(heads)
        ]
        for i in range(1, 4):
            arrived(i)
        query = raw * inv_rms
        key = total(1) * inv_rms * (dh ** (-0.5))
        key_buf[...] = key
        dots, normers = [], []
        for h in range(heads):
            lanes = slice(h * dh, (h + 1) * dh)
            qh, kh = query[:, lanes], key[:, lanes]
            n1 = keeps[h] * normer_buf[b, :, h, :] + writes[h] * kh
            normer_out[b, :, h, :] = n1
            dots.append(jnp.sum(kh * qh, axis=1, keepdims=True))
            normers.append(jnp.sum(n1 * qh, axis=1, keepdims=True))
        value = total(2) * inv_rms
        normed = []
        for h in range(heads):
            lanes = slice(h * dh, (h + 1) * dh)
            written = writes[h] * value[:, lanes]
            written_buf[:, lanes] = written
            numer = keeps[h] * reads[h] + written * dots[h]
            readout = numer / jnp.maximum(jnp.abs(normers[h]), 1.0)
            one = readout * lax.rsqrt(jnp.mean(readout * readout, axis=1, keepdims=True) + EPSILON)
            normed.append(one * head_buf[b : b + 1, lanes])
        outgate = total(3) * inv_rms
        for h in range(heads):
            lanes = slice(h * dh, (h + 1) * dh)
            gate = 1.0 / (1.0 + jnp.exp(-outgate[:, lanes]))
            gated_all[b, own, lanes] = (gate * normed[h]).astype(BF16)

        spread = {}
        reach = sorted(range(1, ndp), key=lambda k: -min(k, ndp - k))
        for k in reach:
            spread[k] = dp_send(
                gated_all.at[b, own],
                gated_all.at[b, own],
                gg_send.at[b, k - 1],
                gg_recv.at[b, k - 1],
                lax.rem(d + k, ndp),
            )
        outs = []
        targets = [
            (zd, lax.rem(x + i, side))
            for zd in list(reversed(z_order)) + [z]
            for i in range(1 if zd is z else 0, side)
        ]
        if b + 1 < blocks:
            def multiply(peer):
                block = row_block(peer, seqs)
                part = jnp.dot(gated_all[b, block, :], proj_buf[b], preferred_element_type=F32)
                out_part[block, :] = part
                for i in range(side):
                    piece = part[:, i * half : (i + 1) * half].astype(BF16)
                    mix_stage[b, i, :, peer] = piece.reshape(outer, few, half)
                for zd, xd in targets:
                    slot = lax.rem(zd * side + xd - t + ntp, ntp) - 1
                    copy = pltpu.make_async_remote_copy(
                        src_ref=mix_stage.at[b, xd, zd, peer],
                        dst_ref=mix_recv.at[b, slot, peer],
                        send_sem=ms_send.at[b, slot, peer],
                        recv_sem=ms_recv.at[b, slot, peer],
                        device_id={"tp": zd * side + xd},
                        device_id_type=MESH,
                    )
                    copy.start()
                    outs.append(copy)

            def landed(gap):
                src = lax.rem(d + ndp - gap, ndp)
                pltpu.make_async_remote_copy(
                    src_ref=gated_all.at[b, own],
                    dst_ref=gated_all.at[b, row_block(src, seqs)],
                    send_sem=gg_send.at[b, gap - 1],
                    recv_sem=gg_recv.at[b, gap - 1],
                    device_id={"dp": src},
                    device_id_type=MESH,
                ).wait_recv()

            multiply(d)
            if pair == 2:
                landed(lax.rem(d - mate + ndp, ndp))
                multiply(mate)
            for step in range(1, ring):
                yp = lax.rem(y + step, ring)
                for i in range(pair):
                    peer = yp * pair + lax.rem(core + i, pair)
                    landed(lax.rem(d - peer + ndp, ndp))
                    multiply(peer)
        else:
            for c in spread.values():
                c.wait_recv()
            part = jnp.dot(gated_all[b], proj_buf[b], preferred_element_type=F32)
            out_stage[...] = part.astype(BF16)
            out_part[...] = part
            for zd, xd in targets:
                dest = zd * side + xd
                slot = lax.rem(dest - t + ntp, ntp) - 1
                copy = pltpu.make_async_remote_copy(
                    src_ref=out_stage.at[row_block(dest, rows)],
                    dst_ref=out_recv.at[slot],
                    send_sem=os_send.at[slot],
                    recv_sem=os_recv.at[slot],
                    device_id={"tp": dest},
                    device_id_type=MESH,
                )
                copy.start()
                outs.append(copy)
        update_cells(b)
        if b + 1 < blocks:
            split_cells(b + 1)
        for c in outs:
            c.wait_recv()
        if b + 1 < blocks:
            columns = pl.ds(pl.multiple_of(x * half, half), half)
            for peer in range(ndp):
                summed = out_part[row_block(peer * outer + z, few), columns]
                for k in range(ntp - 1):
                    summed = summed + mix_recv[b, k, peer].astype(F32)
                mixed[b, x, z, peer] = summed.astype(BF16)
            gather = gather_start(b + 1)
        else:
            summed = out_part[mine, :]
            for k in range(ntp - 1):
                summed = summed + out_recv[k].astype(F32)
            final_out[...] = summed.astype(BF16)
        for c in sends + outs:
            c.wait_send()


def store_kernel(rows, cell, normer, stab, rows_out, cell_out, normer_out, stab_out, cell_sem, sems):
    blocks, seqs = cell.shape[0], cell.shape[1]
    parts = cell_sem.shape[1]
    step = seqs // parts
    copies = [
        pltpu.make_async_copy(
            cell.at[b, i * step : (i + 1) * step],
            cell_out.at[b, i * step : (i + 1) * step],
            cell_sem.at[b, i],
        )
        for b in range(blocks)
        for i in range(parts)
    ]
    for i, (src, dst) in enumerate(((rows, rows_out), (normer, normer_out), (stab, stab_out))):
        copies.append(pltpu.make_async_copy(src, dst, sems.at[i]))
    for c in copies:
        c.start()
    for c in copies:
        c.wait()


def per_device(ntp, ndp, *args):
    (tokens, wq, wk, wv, wo, wig, wfg, norm_gain, head_gain, proj, cell, normer, stab) = args
    blocks, width, inner = wq.shape
    all_heads = wig.shape[2]
    seqs, heads, dh = cell.shape[1], cell.shape[2], cell.shape[3]
    rows = tokens.shape[0]
    pair = 2 if ndp % 2 == 0 else 1
    ring = ndp // pair
    more = max(ring - 1, 1)
    passed = max(blocks - 1, 1)
    outer, side = split_axis(ntp)
    few = seqs // outer
    wig, wfg, stab = (jnp.swapaxes(a, 1, 2) for a in (wig, wfg, stab))
    batch = rows * ntp
    lanes = -(-heads // 128) * 128
    gate_rows = -(-(2 * heads + 1) // 8) * 8
    vmem = pl.BlockSpec(memory_space=pltpu.VMEM)
    hbm = pl.BlockSpec(memory_space=pltpu.HBM)
    dma = pltpu.SemaphoreType.DMA
    results = pl.pallas_call(
        functools.partial(step_kernel, ntp, ndp),
        out_shape=(
            pltpu.VMEM(tokens.shape, BF16),
            pltpu.VMEM(cell.shape, F32),
            pltpu.VMEM(normer.shape, F32),
            pltpu.VMEM(stab.shape, F32),
        ),
        in_specs=[hbm] * 13,
        out_specs=(vmem,) * 4,
        scratch_shapes=[
            pltpu.VMEM((blocks, 4, width, inner), BF16),
            pltpu.VMEM((blocks, all_heads, width), BF16),
            pltpu.VMEM((blocks, all_heads, width), BF16),
            pltpu.VMEM(proj.shape, BF16),
            pltpu.VMEM((seqs, inner), F32),
            pltpu.VMEM((seqs, inner), F32),
            pltpu.VMEM((seqs, lanes), F32),
            dma,
            dma((4,)),
            pltpu.VMEM(norm_gain.shape, F32),
            pltpu.VMEM(head_gain.shape, F32),
            pltpu.VMEM(normer.shape, F32),
            pltpu.VMEM(stab.shape, F32),
            pltpu.VMEM((2, seqs * dh, heads * dh), BF16),
            pltpu.VMEM((batch, width), BF16),
            pltpu.VMEM((passed, side, outer, ndp, few, width // side), BF16),
            pltpu.VMEM((batch, width), BF16),
            pltpu.VMEM((4, ndp, outer, few, inner), F32),
            pltpu.VMEM((passed, 4, outer, ndp, few, inner), F32),
            pltpu.VMEM((blocks, gate_rows, batch), F32),
            pltpu.VMEM((blocks, ndp - 1, gate_rows, batch), F32),
            pltpu.VMEM((batch, gate_rows), F32),
            pltpu.VMEM((blocks, 4, ring, outer, few, inner), F32),
            pltpu.VMEM((blocks, 4, more, outer, few, inner), F32),
            pltpu.VMEM((blocks, 4, more, outer, few, inner), F32),
            pltpu.VMEM((2, more, seqs, inner), BF16),
            pltpu.VMEM((2, more, seqs, inner), BF16),
            pltpu.VMEM((blocks, batch, inner), BF16),
            pltpu.VMEM((batch, width), F32),
            pltpu.VMEM((batch, width), BF16),
            pltpu.VMEM((ntp - 1, rows, width), BF16),
            pltpu.VMEM((passed, side, outer, ndp, few, width // side), BF16),
            pltpu.VMEM((passed, ntp - 1, ndp, few, width // side), BF16),
            dma((blocks, 7)),
            dma((blocks,)),
            dma((blocks, ntp - 1)),
            dma((blocks, ntp - 1)),
            dma((blocks, 4, ring)),
            dma((blocks, 4, ring)),
            dma((blocks, 4, more)),
            dma((blocks, 4, more)),
            dma((blocks, ndp - 1)),
            dma((blocks, ndp - 1)),
            dma((blocks, ndp - 1)),
            dma((blocks, ndp - 1)),
            dma((ntp - 1,)),
            dma((ntp - 1,)),
            dma((passed, ntp - 1, ndp)),
            dma((passed, ntp - 1, ndp)),
        ],
        compiler_params=pltpu.CompilerParams(
            collective_id=0, has_side_effects=True, vmem_limit_bytes=40 << 20
        ),
    )(
        *[
            pltpu.with_memory_space_constraint(a, pltpu.HBM)
            for a in (
                tokens, wq, wk, wv, wo, wig, wfg, norm_gain, head_gain, proj, cell, normer, stab
            )
        ]
    )

    shapes = tuple(jax.ShapeDtypeStruct(a.shape, a.dtype) for a in results)
    rows_out, cell_out, normer_out, stab_out = pl.pallas_call(
        store_kernel,
        out_shape=shapes,
        in_specs=[vmem] * 4,
        out_specs=(hbm,) * 4,
        scratch_shapes=[dma((blocks, math.gcd(seqs, 8))), dma((3,))],
        compiler_params=pltpu.CompilerParams(vmem_limit_bytes=1 << 20),
    )(*results)
    return rows_out, cell_out, normer_out, jnp.swapaxes(stab_out, 1, 2)


def solution(mesh):
    return jax.shard_map(
        functools.partial(per_device, mesh.shape["tp"], mesh.shape["dp"]),
        mesh=mesh,
        in_specs=(
            P("tp", "dp"),
            P(None, "dp", "tp"),
            P(None, "dp", "tp"),
            P(None, "dp", "tp"),
            P(None, "dp", "tp"),
            P(),
            P(),
            P(None, "dp"),
            P(None, "tp"),
            P(None, "tp", "dp"),
            P(None, "dp", "tp", None, None),
            P(None, "dp", "tp", None),
            P(None, "dp", "tp"),
        ),
        out_specs=(
            P("tp", "dp"),
            P(None, "dp", "tp", None, None),
            P(None, "dp", "tp", None),
            P(None, "dp", "tp"),
        ),
        check_vma=False,
    )
```
